32 devices in a mesh: dp: 4 (over y, x), kv: 4 (over z), tp: 2 (over core).
Axes of the slice: x: 2, y: 2, z: 4, core: 2. Of those that a mesh axis runs over, the one named last changes fastest.
Arguments:
- stream: bfloat16 [32, 2048], P('dp', ('kv', 'tp')), parts along dimension 0, may hold values from -40 to 40
- old_state: float32 [32, 8, 64, 128], P(('dp', 'kv'), 'tp'), parts along dimension 0, may hold values from -6 to 6
- decay_amounts: float32 [32, 512], P(('dp', 'kv'), 'tp'), parts along dimension 0, may hold values from 0.003 to 1
- first_gain: float32 [2048], replicated, may hold values from 0.1 to 1.9
- first_gate: bfloat16 [2048, 5632], P(None, ('kv', 'tp')), may hold values from -0.125 to 0.125
- first_up: bfloat16 [2048, 5632], P(None, ('kv', 'tp')), may hold values from -0.125 to 0.125
- first_down: bfloat16 [5632, 2048], P(('kv', 'tp')), may hold values from -0.078125 to 0.078125
- mixer_gain: float32 [2048], P('kv'), may hold values from 0.1 to 1.9
- query_weight: bfloat16 [2048, 512], P('kv', 'tp'), may hold values from -0.125 to 0.125
- key_weight: bfloat16 [2048, 512], P('kv', 'tp'), may hold values from -0.125 to 0.125
- decay_weight: bfloat16 [2048, 512], P('kv', 'tp'), may hold values from -0.5 to 0.5
- value_weight: bfloat16 [2048, 1024], P('kv', 'tp'), may hold values from -0.125 to 0.125
- output_gate_weight: bfloat16 [2048, 1024], P('kv', 'tp'), may hold values from -0.125 to 0.125
- head_gain: float32 [1024], P('tp'), may hold values from 0.1 to 1.9
- output_weight: bfloat16 [1024, 2048], P('tp', 'kv'), may hold values from -0.1875 to 0.1875
- second_gain: float32 [2048], replicated, may hold values from 0.1 to 1.9
- second_gate: bfloat16 [2048, 5632], P(None, ('kv', 'tp')), may hold values from -0.125 to 0.125
- second_up: bfloat16 [2048, 5632], P(None, ('kv', 'tp')), may hold values from -0.125 to 0.125
- second_down: bfloat16 [5632, 2048], P(('kv', 'tp')), may hold values from -0.078125 to 0.078125
Outputs:
- mixed_stream: bfloat16 [32, 2048], P('dp', ('kv', 'tp')), parts along dimension 0
- new_state: float32 [32, 8, 64, 128], P(('dp', 'kv'), 'tp'), parts along dimension 0
The draws below stay inside these ranges and needn't reach their ends.
There are 4 independent parts, one for each index of `dp`. The reference program is written for one: setup_inputs(seed, part) draws one part's arguments, and reference() takes and returns one part's arrays. A program takes and returns all parts, laid end to end along the dimension named above; an argument that names none is the same for every part. Nothing has to cross between parts.
All inputs are finite; a program needn't handle non-finite values.
Results may differ from the reference program's by a relative error of at most 0.007.
Values may be sent and summed in bfloat16 or wider, within the bound.
No kernel may reach another device: no remote copies, remote signals or barrier semaphores. Data moves between devices by JAX's collectives and lax.ppermute only.
A program may use at most 64 MiB of HBM per device.

```python
import math
import jax
import jax.numpy as jnp
from jax import lax

D = 2048
FF = 5632
HEAD_TOTAL = 8
KEY_CHANNELS = 64
VALUE_DIM = 128
SEQS = 8
N_TP = 2


def draw_stream(key, part):
    first_key = jax.random.fold_in(key, 11)
    second_key = jax.random.fold_in(key, 12)
    columns = jnp.arange(D, dtype=jnp.float32)
    rising = 1.0 + 2.0 * columns / D
    rough = jnp.exp(jax.random.uniform(second_key, (D,), jnp.float32, -0.4, 0.4))
    base = jnp.clip(jax.random.normal(first_key, (SEQS, D), jnp.float32), -4.0, 4.0)
    return (base * rising * rough).astype(jnp.bfloat16)


def block_levels(stream_key, shape, cuts, smallest, largest):
    gain = 1.0
    for position, parts in cuts:
        steps = jax.random.uniform(jax.random.fold_in(jax.random.fold_in(stream_key, 6), position), (parts,), jnp.float32, smallest / len(cuts), largest / len(cuts))
        gain = gain * jnp.repeat(jnp.exp(steps), shape[position] // parts).reshape((-1,) + (1,) * (len(shape) - 1 - position))
    return gain


def bell_draw(stream_key, extent, scale, limit, cuts=(), kind=jnp.bfloat16):
    level = block_levels(stream_key, extent, cuts, -0.22, 0.18) if cuts else 1.0
    array = jax.random.normal(stream_key, extent, jnp.float32) * scale * level
    return jnp.minimum(jnp.maximum(array, -limit), limit).astype(kind)


def setup_inputs(seed: int = 0, part: int = 0) -> dict:
    arg_keys = jax.random.split(jax.random.key(seed), 20)
    part_keys = jax.random.split(jax.random.fold_in(arg_keys[19], part), 20)
    stream = draw_stream(jax.random.fold_in(jax.random.fold_in(arg_keys[19], part), 71), part)
    old_state = bell_draw(part_keys[1], (SEQS, HEAD_TOTAL, KEY_CHANNELS, VALUE_DIM), 1.0, 6.0, ((0, 4), (1, 2)), jnp.float32)
    decay_amounts = jnp.clip(jnp.exp(math.log(1.0) - 5.809143 * jax.random.uniform(part_keys[2], (SEQS, HEAD_TOTAL * KEY_CHANNELS), jnp.float32) ** block_levels(part_keys[2], (SEQS, HEAD_TOTAL * KEY_CHANNELS), ((0, 4), (1, 2)), -0.2, 0.2)), 0.003, 1.0)
    first_gain = jnp.clip(1.0 + 0.18 * jax.random.normal(arg_keys[3], (D,), jnp.float32), 0.1, 1.9)
    first_gate = bell_draw(arg_keys[4], (D, FF), D ** -0.5, 0.125, ((1, 8),))
    first_up = bell_draw(arg_keys[5], (D, FF), D ** -0.5, 0.125, ((1, 8),))
    first_down = bell_draw(arg_keys[6], (FF, D), FF ** -0.5, 0.078125, ((0, 8),))
    mixer_gain = jnp.clip(1.0 + 0.18 * jax.random.normal(arg_keys[7], (D,), jnp.float32), 0.1, 1.9)
    query_weight = bell_draw(arg_keys[8], (D, HEAD_TOTAL * KEY_CHANNELS), D ** -0.5, 0.125, ((0, 4), (1, 2)))
    key_weight = bell_draw(arg_keys[9], (D, HEAD_TOTAL * KEY_CHANNELS), D ** -0.5, 0.125, ((0, 4), (1, 2)))
    decay_weight = bell_draw(arg_keys[10], (D, HEAD_TOTAL * KEY_CHANNELS), (D // 16) ** -0.5, 0.5, ((0, 4), (1, 2)))
    value_weight = bell_draw(arg_keys[11], (D, HEAD_TOTAL * VALUE_DIM), D ** -0.5, 0.125, ((0, 4), (1, 2)))
    output_gate_weight = bell_draw(arg_keys[12], (D, HEAD_TOTAL * VALUE_DIM), D ** -0.5, 0.125, ((0, 4), (1, 2)))
    head_gain = jnp.clip(1.0 + 0.18 * jax.random.normal(arg_keys[13], (HEAD_TOTAL * VALUE_DIM,), jnp.float32), 0.1, 1.9)
    output_weight = bell_draw(arg_keys[14], (HEAD_TOTAL * VALUE_DIM, D), (HEAD_TOTAL * VALUE_DIM) ** -0.5, 0.1875, ((0, 2), (1, 4)))
    second_gain = jnp.clip(1.0 + 0.18 * jax.random.normal(arg_keys[15], (D,), jnp.float32), 0.1, 1.9)
    second_gate = bell_draw(arg_keys[16], (D, FF), D ** -0.5, 0.125, ((1, 8),))
    second_up = bell_draw(arg_keys[17], (D, FF), D ** -0.5, 0.125, ((1, 8),))
    second_down = bell_draw(arg_keys[18], (FF, D), FF ** -0.5, 0.078125, ((0, 8),))
    return {"stream": stream, "old_state": old_state, "decay_amounts": decay_amounts, "first_gain": first_gain, "first_gate": first_gate, "first_up": first_up, "first_down": first_down, "mixer_gain": mixer_gain, "query_weight": query_weight, "key_weight": key_weight, "decay_weight": decay_weight, "value_weight": value_weight, "output_gate_weight": output_gate_weight, "head_gain": head_gain, "output_weight": output_weight, "second_gain": second_gain, "second_gate": second_gate, "second_up": second_up, "second_down": second_down}


EPSILON = 1e-06
GATE_SOFTNESS = 16.0

def row_scale_of(rows):
    wide = rows.astype(jnp.float32)
    return lax.rsqrt(lax.optimization_barrier(jnp.mean(wide * wide, axis=-1, keepdims=True)) + EPSILON)

def half_block(stream, norm_gain, w_gate, w_up, w_down):
    row_scale = row_scale_of(stream)
    scaled = (stream.astype(jnp.float32) * norm_gain).astype(jnp.bfloat16)
    gate_part = jnp.dot(scaled, w_gate, preferred_element_type=jnp.float32) * row_scale
    up_part = jnp.dot(scaled, w_up, preferred_element_type=jnp.float32) * row_scale
    hidden = (jax.nn.silu(gate_part) * up_part).astype(jnp.bfloat16)
    result = stream.astype(jnp.float32) + 0.5 * jnp.dot(hidden, w_down, preferred_element_type=jnp.float32)
    return result.astype(jnp.bfloat16)

def reference(stream, old_state, decay_amounts, first_gain, first_gate, first_up, first_down, mixer_gain, query_weight, key_weight, decay_weight, value_weight, output_gate_weight, head_gain, output_weight, second_gain, second_gate, second_up, second_down):
    middle = half_block(stream, first_gain, first_gate, first_up, first_down)
    row_scale = row_scale_of(middle)
    scaled = (middle.astype(jnp.float32) * mixer_gain).astype(jnp.bfloat16)

    def project(weight_block):
        return jnp.dot(scaled, weight_block, preferred_element_type=jnp.float32) * row_scale
    sequence_count = stream.shape[0]
    query = (project(query_weight) * KEY_CHANNELS ** (-0.5)).reshape(sequence_count, HEAD_TOTAL, KEY_CHANNELS)
    keys = project(key_weight).reshape(sequence_count, HEAD_TOTAL, KEY_CHANNELS)
    gate_logits = project(decay_weight).reshape(sequence_count, HEAD_TOTAL, KEY_CHANNELS)
    values = project(value_weight).reshape(sequence_count, HEAD_TOTAL, VALUE_DIM)
    out_gate = project(output_gate_weight)
    decay_logarithm = jax.nn.log_sigmoid(gate_logits) / GATE_SOFTNESS - decay_amounts.reshape(sequence_count, HEAD_TOTAL, KEY_CHANNELS)
    new_state = jnp.exp(decay_logarithm)[..., None] * old_state + keys[..., None] * values[:, :, None, :]
    readout = jnp.einsum('bhk,bhkv->bhv', query, new_state, precision=lax.Precision.HIGHEST)
    normed = readout * lax.rsqrt(lax.optimization_barrier(jnp.mean(readout * readout, axis=-1, keepdims=True)) + EPSILON)
    mixed_heads = (normed.reshape(sequence_count, HEAD_TOTAL * VALUE_DIM) * head_gain * jax.nn.silu(out_gate)).astype(jnp.bfloat16)
    group_width = HEAD_TOTAL * VALUE_DIM // N_TP
    attention_out = jnp.zeros((sequence_count, D), jnp.float32)
    for group in range(N_TP):
        partial_out = jnp.dot(mixed_heads[:, group * group_width:(group + 1) * group_width], output_weight[group * group_width:(group + 1) * group_width], preferred_element_type=jnp.float32).astype(jnp.bfloat16)
        attention_out = attention_out + lax.optimization_barrier(partial_out).astype(jnp.float32)
    after = (middle.astype(jnp.float32) + attention_out).astype(jnp.bfloat16)
    mixed_stream = half_block(after, second_gain, second_gate, second_up, second_down)
    return (mixed_stream, new_state)
```

```python
import functools
import jax
import jax.numpy as jnp
from jax import lax
from jax.sharding import PartitionSpec as P

EPSILON = 1e-06
GATE_SOFTNESS = 16.0
f32 = jnp.float32
bf16 = jnp.bfloat16


def swap(x, axis, size, shift):
    return lax.ppermute(x, axis, [(j, j ^ shift) for j in range(size)])


def unscramble(pieces, index):
    stacked = jnp.stack(pieces)
    order = jnp.arange(len(pieces)) ^ index
    out = []
    for j in range(len(pieces)):
        choice = pieces[0]
        for s in range(1, len(pieces)):
            choice = jnp.where(order[j] == s, pieces[s], choice)
        out.append(choice)
    return out


def gather_kv(x, n_kv):
    pieces = [x] + [swap(x, "kv", n_kv, s) for s in range(1, n_kv)]
    return unscramble(pieces, lax.axis_index("kv"))


def scatter_sum_kv(blocks, n_kv):
    kv = lax.axis_index("kv")
    total = blocks(kv)
    for s in range(1, n_kv):
        total = total + swap(blocks(kv ^ s), "kv", n_kv, s)
    return total


def pair_order(mine, other):
    first = lax.axis_index("tp") == 0
    return jnp.where(first, mine, other), jnp.where(first, other, mine)


def ffn(wide, norm_gain, w_gate, w_up, w_down):
    wide = wide.astype(f32)
    scaled = (wide * norm_gain).astype(bf16)
    gate_acc = jnp.dot(scaled, w_gate, preferred_element_type=f32)
    up_acc = jnp.dot(scaled, w_up, preferred_element_type=f32)
    row_scale = lax.rsqrt(jnp.mean(wide * wide, axis=1) + EPSILON)[:, None]
    hidden = (jax.nn.silu(gate_acc * row_scale) * (up_acc * row_scale)).astype(bf16)
    return jnp.dot(hidden, w_down, preferred_element_type=f32)


def body(n_kv, n_tp,
    stream, old_state, decay_amounts, first_gain, first_gate, first_up, first_down, mixer_gain,
    query_weight, key_weight, decay_weight, value_weight, output_gate_weight, head_gain, output_weight,
    second_gain, second_gate, second_up, second_down,
):
    rows, own = stream.shape
    width = own * n_tp
    kv = lax.axis_index("kv")
    tp = lax.axis_index("tp")
    chip_cols = jnp.concatenate(pair_order(stream, swap(stream, "tp", n_tp, 1)), axis=1)
    wide = jnp.concatenate(gather_kv(chip_cols, n_kv), axis=1)
    partial_out = ffn(wide, first_gain, first_gate, first_up, first_down)
    summed = scatter_sum_kv(
        lambda j: lax.dynamic_slice_in_dim(partial_out, j * width, width, 1), n_kv
    )
    summed = summed + swap(summed, "tp", n_tp, 1)
    middle = (chip_cols.astype(f32) + 0.5 * summed).astype(bf16)
    middle_wide = middle.astype(f32)
    scaled = (middle_wide * mixer_gain).astype(bf16)
    dots = [
        jnp.dot(scaled, w, preferred_element_type=f32)
        for w in (query_weight, key_weight, decay_weight, value_weight, output_gate_weight)
    ]
    squares = jnp.broadcast_to(jnp.sum(middle_wide * middle_wide, axis=1, keepdims=True), (rows, 128))
    parts = jnp.concatenate(dots + [squares], axis=1)
    local_rows, local_heads, key_dim, value_dim = old_state.shape
    sums = scatter_sum_kv(
        lambda j: lax.dynamic_slice_in_dim(parts, j * local_rows, local_rows, 0), n_kv
    )
    nk, nv = local_heads * key_dim, local_heads * value_dim
    row_scale = lax.rsqrt(sums[:, -1:] / (width * n_kv) + EPSILON)
    query = (sums[:, :nk] * row_scale * key_dim ** (-0.5)).reshape(local_rows, local_heads, key_dim)
    keys = (sums[:, nk:2 * nk] * row_scale).reshape(local_rows, local_heads, key_dim)
    gate_logits = (sums[:, 2 * nk:3 * nk] * row_scale).reshape(local_rows, local_heads, key_dim)
    values = (sums[:, 3 * nk:3 * nk + nv] * row_scale).reshape(local_rows, local_heads, value_dim)
    outgate = sums[:, 3 * nk + nv:3 * nk + 2 * nv] * row_scale
    decay_logarithm = jax.nn.log_sigmoid(gate_logits) / GATE_SOFTNESS - decay_amounts.reshape(
        local_rows, local_heads, key_dim
    )
    new_state = (
        jnp.exp(decay_logarithm)[..., None] * old_state + keys[..., None] * values[:, :, None, :]
    )
    readout = jnp.einsum("bhk,bhkv->bhv", query, new_state, precision=lax.Precision.HIGHEST)
    normed = readout * lax.rsqrt(jnp.mean(readout * readout, axis=-1, keepdims=True) + EPSILON)
    mixed_heads = (
        normed.reshape(local_rows, nv) * head_gain * jax.nn.silu(outgate)
    ).astype(bf16)
    all_heads = jnp.concatenate(gather_kv(mixed_heads, n_kv), axis=0)
    projected = jnp.dot(all_heads, output_weight, preferred_element_type=f32).astype(bf16)
    projected = lax.optimization_barrier(projected)
    attention_out = projected.astype(f32) + swap(projected, "tp", n_tp, 1).astype(f32)
    after = (middle_wide + attention_out).astype(bf16)
    wide = jnp.concatenate(gather_kv(after, n_kv), axis=1)
    partial_out = ffn(wide, second_gain, second_gate, second_up, second_down)
    by_core = partial_out.reshape(rows, n_kv, n_tp, own)
    halves = by_core[:, :, 0], by_core[:, :, 1]
    mine = jnp.where(tp == 0, halves[0], halves[1])
    theirs = jnp.where(tp == 0, halves[1], halves[0])
    mine = mine + swap(theirs, "tp", n_tp, 1)
    summed = scatter_sum_kv(
        lambda j: lax.dynamic_index_in_dim(mine, j, 1, keepdims=False), n_kv
    )
    after_own = jnp.where(tp == 0, after[:, :own], after[:, own:])
    mixed_stream = (after_own.astype(f32) + 0.5 * summed).astype(bf16)
    return (mixed_stream, new_state)


def half_block(stream, norm_gain, w_gate, w_up, w_down):
    wide = lax.all_gather(stream, ("kv", "tp"), axis=1, tiled=True).astype(jnp.float32)
    scaled = (wide * norm_gain).astype(jnp.bfloat16)
    gate_acc = jnp.dot(scaled, w_gate, preferred_element_type=jnp.float32)
    up_acc = jnp.dot(scaled, w_up, preferred_element_type=jnp.float32)
    square_acc = jnp.sum(wide * wide, axis=1)
    row_scale = lax.rsqrt(square_acc / norm_gain.shape[0] + EPSILON)[:, None]
    hidden = (jax.nn.silu(gate_acc * row_scale) * (up_acc * row_scale)).astype(jnp.bfloat16)
    partial_out = jnp.dot(hidden, w_down, preferred_element_type=jnp.float32)
    summed = lax.psum_scatter(partial_out, ("kv", "tp"), scatter_dimension=1, tiled=True)
    return (stream.astype(jnp.float32) + 0.5 * summed).astype(jnp.bfloat16)


def wide_body(
    stream,
    old_state,
    decay_amounts,
    first_gain,
    first_gate,
    first_up,
    first_down,
    mixer_gain,
    query_weight,
    key_weight,
    decay_weight,
    value_weight,
    output_gate_weight,
    head_gain,
    output_weight,
    second_gain,
    second_gate,
    second_up,
    second_down,
):
    middle = half_block(stream, first_gain, first_gate, first_up, first_down)
    paired_cols = lax.all_gather(middle, "tp", axis=1, tiled=True)
    wide_cols = paired_cols.astype(jnp.float32)
    scaled = (wide_cols * mixer_gain).astype(jnp.bfloat16)
    query_part = jnp.dot(scaled, query_weight, preferred_element_type=jnp.float32)
    key_part = jnp.dot(scaled, key_weight, preferred_element_type=jnp.float32)
    decay_part = jnp.dot(scaled, decay_weight, preferred_element_type=jnp.float32)
    value_part = jnp.dot(scaled, value_weight, preferred_element_type=jnp.float32)
    outgate_part = jnp.dot(scaled, output_gate_weight, preferred_element_type=jnp.float32)
    local_rows = old_state.shape[0]
    local_heads = old_state.shape[1]
    key_dim = old_state.shape[2]
    value_dim = old_state.shape[3]
    query_sum, key_sum, decay_sum, value_sum, outgate_sum, own_squares = (
        lax.psum_scatter(query_part, "kv", scatter_dimension=0, tiled=True),
        lax.psum_scatter(key_part, "kv", scatter_dimension=0, tiled=True),
        lax.psum_scatter(decay_part, "kv", scatter_dimension=0, tiled=True),
        lax.psum_scatter(value_part, "kv", scatter_dimension=0, tiled=True),
        lax.psum_scatter(outgate_part, "kv", scatter_dimension=0, tiled=True),
        lax.psum_scatter(
            jnp.sum(wide_cols * wide_cols, axis=1), "kv", scatter_dimension=0, tiled=True
        ),
    )
    row_scale = lax.rsqrt(own_squares / (wide_cols.shape[1] * lax.axis_size("kv")) + EPSILON)[:, None]
    query = (query_sum * row_scale * key_dim ** (-0.5)).reshape(local_rows, local_heads, key_dim)
    keys = (key_sum * row_scale).reshape(local_rows, local_heads, key_dim)
    gate_logits = (decay_sum * row_scale).reshape(local_rows, local_heads, key_dim)
    values = (value_sum * row_scale).reshape(local_rows, local_heads, value_dim)
    decay_logarithm = jax.nn.log_sigmoid(gate_logits) / GATE_SOFTNESS - decay_amounts.reshape(
        local_rows, local_heads, key_dim
    )
    new_state = (
        jnp.exp(decay_logarithm)[..., None] * old_state + keys[..., None] * values[:, :, None, :]
    )
    readout = jnp.einsum("bhk,bhkv->bhv", query, new_state, precision=lax.Precision.HIGHEST)
    normed = readout * lax.rsqrt(jnp.mean(readout * readout, axis=-1, keepdims=True) + EPSILON)
    mixed_heads = (
        normed.reshape(local_rows, local_heads * value_dim)
        * head_gain
        * jax.nn.silu(outgate_sum * row_scale)
    ).astype(jnp.bfloat16)
    projected = jnp.dot(
        lax.all_gather(mixed_heads, "kv", axis=0, tiled=True),
        output_weight,
        preferred_element_type=jnp.float32,
    ).astype(jnp.bfloat16)
    attention_out = lax.psum_scatter(
        lax.optimization_barrier(projected).astype(jnp.float32).astype(jnp.bfloat16),
        "tp",
        scatter_dimension=1,
        tiled=True,
    ).astype(jnp.float32)
    after = (middle.astype(jnp.float32) + attention_out).astype(jnp.bfloat16)
    mixed_stream = half_block(after, second_gain, second_gate, second_up, second_down)
    return (mixed_stream, new_state)


def solution(mesh):
    n_kv, n_tp = mesh.shape["kv"], mesh.shape["tp"]
    few = n_kv <= 8 and n_kv & (n_kv - 1) == 0 and n_tp == 2
    program = functools.partial(body, n_kv, n_tp) if few else wide_body
    in_specs = (
        P("dp", ("kv", "tp")),
        P(("dp", "kv"), "tp", None, None),
        P(("dp", "kv"), "tp"),
        P(),
        P(None, ("kv", "tp")),
        P(None, ("kv", "tp")),
        P(("kv", "tp"), None),
        P("kv"),
        P("kv", "tp"),
        P("kv", "tp"),
        P("kv", "tp"),
        P("kv", "tp"),
        P("kv", "tp"),
        P("tp"),
        P("tp", "kv"),
        P(),
        P(None, ("kv", "tp")),
        P(None, ("kv", "tp")),
        P(("kv", "tp"), None),
    )
    out_specs = (P("dp", ("kv", "tp")), P(("dp", "kv"), "tp", None, None))
    return jax.shard_map(program, mesh=mesh, in_specs=in_specs, out_specs=out_specs, check_vma=False)
```

```python
import functools

import jax
import jax.numpy as jnp
from jax import lax
from jax.experimental import pallas as pl
from jax.experimental.pallas import tpu as pltpu
from jax.sharding import PartitionSpec as P


EPSILON = 1e-06
GATE_SOFTNESS = 16.0
f32 = jnp.float32
bf16 = jnp.bfloat16
LANES = 128


def shape(dims, dtype=f32):
    return jax.ShapeDtypeStruct(tuple(dims), dtype)


def call(kernel, outs, *args, scratch=(), flops=0, limit=4, moved=None):
    vmem = pl.BlockSpec(memory_space=pltpu.VMEM)
    moved = moved or sum(a.size * a.dtype.itemsize for a in args)
    return pl.pallas_call(
        kernel,
        out_shape=outs,
        in_specs=[vmem] * len(args),
        out_specs=jax.tree.map(lambda _: vmem, outs),
        scratch_shapes=list(scratch),
        cost_estimate=pl.CostEstimate(flops=flops, bytes_accessed=moved, transcendentals=0),
        compiler_params=pltpu.CompilerParams(vmem_limit_bytes=limit << 20),
    )(*args)


def swap(x, axis, size, shift):
    return lax.ppermute(x, axis, [(j, j ^ shift) for j in range(size)])


def send_kv(blocks, n_kv):
    got = []
    for s in range(1, n_kv):
        got.append(swap(blocks[s - 1], "kv", n_kv, s))
    return got


def silu(x):
    return x / (1.0 + jnp.exp(-x))


def dot_t(a, b):
    return lax.dot_general(a, b, (((1,), (1,)), ((), ())), preferred_element_type=f32)


def dot(a, b):
    return jnp.dot(a, b, preferred_element_type=f32)


def add_pieces(pieces, order, side, gain, w_gate, w_up, gate, up, square):
    kv = lax.axis_index("kv")
    pair = w_gate.shape[1] // lax.axis_size("kv")
    for piece, s in zip(pieces, order):
        width = piece.shape[1]
        start = (kv ^ s) * pair
        if width < pair:
            start = start + side * width
        cols = pl.ds(pl.multiple_of(start, width), width)
        wide = piece.astype(f32)
        scaled = (wide * gain[:, cols]).astype(bf16)
        one = dot_t(scaled, w_gate[:, cols])
        two = dot_t(scaled, w_up[:, cols])
        gate = one if gate is None else gate + one
        up = two if up is None else up + two
        squares = jnp.sum(wide * wide, axis=1, keepdims=True)
        square = squares if square is None else square + squares
    return gate, up, square


def hidden_of(gate, up, square, depth):
    scale = lax.rsqrt(square / depth + EPSILON)
    return (silu(gate * scale) * (up * scale)).astype(bf16)


def copy_kernel(x, out):
    out[...] = x[...]


def pack_kernel(*refs):
    *ins, out = refs
    for s, ref in enumerate(ins):
        out[s] = ref[...]


def up_own_kernel(x, gain, w_gate, w_up, acc, sq):
    n = x.shape[0]
    gate, up, square = add_pieces(
        [x[s] for s in range(n)], range(n), lax.axis_index("tp"), gain, w_gate, w_up, None, None, None
    )
    acc[0], acc[1] = gate, up
    sq[...] = jnp.broadcast_to(square, sq.shape)


def first_kernel(x, gain, w_gate, w_up, acc, sq, w_down, *outs):
    n = x.shape[0]
    gate, up, square = add_pieces(
        [x[s] for s in range(n)], range(n), 1 - lax.axis_index("tp"), gain, w_gate, w_up,
        acc[0], acc[1], sq[:, :1],
    )
    hidden = hidden_of(gate, up, square, w_gate.shape[1])
    kv = lax.axis_index("kv")
    for s, out in enumerate(outs):
        width = out.shape[1]
        cols = pl.ds(pl.multiple_of((kv ^ s) * width, width), width)
        out[...] = dot(hidden, w_down[:, cols])


def sum_kernel(*refs):
    *ins, out = refs
    total = ins[0][...]
    for ref in ins[1:]:
        total = total + ref[...]
    out[...] = total


def project_kernel(mine, other, x_own, x_other, gain, wq, wk, wz, wv, wo, middle, *rest):
    *outs, scr = rest
    kv = lax.axis_index("kv")
    lower = lax.axis_index("tp") == 0
    own, far = x_own[0].astype(f32), x_other[0].astype(f32)
    stream = jnp.concatenate(
        [jnp.where(lower, own, far), jnp.where(lower, far, own)], axis=1
    )
    mid = (stream + 0.5 * (mine[...] + other[...])).astype(bf16)
    middle[...] = mid
    wide = mid.astype(f32)
    scaled = (wide * gain[...]).astype(bf16)
    n, rows = scr.shape[:2]
    squares = jnp.sum(wide * wide, axis=1, keepdims=True)
    parts = [dot(scaled, w[...]) for w in (wq, wk, wz, wv, wo)]
    parts.append(jnp.broadcast_to(squares, (wide.shape[0], LANES)))
    at = 0
    for part in parts:
        for j in range(n):
            scr[j, :, at:at + part.shape[1]] = part[j * rows:(j + 1) * rows]
        at += part.shape[1]
    for s, out in enumerate(outs):
        out[...] = scr[kv ^ s]


def state_kernel(depth, *refs):
    *ins, old, amounts, head_gain, new, mixed = refs
    rows, heads, keys, values = old.shape
    nk, nv = heads * keys, heads * values
    total = ins[0][...]
    for ref in ins[1:]:
        total = total + ref[...]
    scale = lax.rsqrt(total[:, -1:] / depth + EPSILON)
    total = total * scale
    query = total[:, :nk] * keys ** (-0.5)
    key = total[:, nk:2 * nk]
    z = total[:, 2 * nk:3 * nk]
    value = total[:, 3 * nk:3 * nk + nv]
    out_gate = total[:, 3 * nk + nv:3 * nk + 2 * nv]
    log_sigmoid = jnp.minimum(z, 0.0) - jnp.log1p(jnp.exp(-jnp.abs(z)))
    decay = jnp.exp(log_sigmoid / GATE_SOFTNESS - amounts[...])
    turned = jnp.concatenate([query, key, decay], axis=0)
    short = -turned.shape[0] % 8
    if short:
        turned = jnp.concatenate([turned, jnp.zeros((short, nk), f32)], axis=0)
    turned = turned.T
    gated = silu(out_gate) * head_gain[...]
    for b in range(rows):
        for h in range(heads):
            at = slice(h * keys, (h + 1) * keys)
            cols = slice(h * values, (h + 1) * values)
            q = turned[at, b:b + 1]
            k = turned[at, rows + b:rows + b + 1]
            d = turned[at, 2 * rows + b:2 * rows + b + 1]
            state = d * old[b, h] + k * value[b:b + 1, cols]
            new[b, h] = state
            readout = jnp.sum(q * state, axis=0, keepdims=True)
            normed = readout * lax.rsqrt(
                jnp.mean(readout * readout, axis=1, keepdims=True) + EPSILON
            )
            mixed[b:b + 1, cols] = (normed * gated[b:b + 1, cols]).astype(bf16)


def output_kernel(*refs):
    *ins, w_out, out, scr = refs
    kv = lax.axis_index("kv")
    for s, ref in enumerate(ins):
        scr[kv ^ s] = ref[...].astype(f32)
    heads = jnp.concatenate([scr[j] for j in range(len(ins))], axis=0)
    out[...] = dot(heads.astype(bf16), w_out[...]).astype(bf16)


def after_kernel(middle, mine, other, after):
    added = mine[...].astype(f32) + other[...].astype(f32)
    after[...] = (middle[...].astype(f32) + added).astype(bf16)


def up_block_kernel(x, gain, w_gate, w_up, acc, sq):
    gate, up, square = add_pieces([x[...]], [0], 0, gain, w_gate, w_up, None, None, None)
    acc[0], acc[1] = gate, up
    sq[...] = jnp.broadcast_to(square, sq.shape)


def second_kernel(*refs):
    *pieces, gain, w_gate, w_up, acc, sq, w_down, mine, theirs = refs
    gate, up, square = add_pieces(
        [p[...] for p in pieces], range(1, len(pieces) + 1), 0, gain, w_gate, w_up,
        acc[0], acc[1], sq[:, :1],
    )
    hidden = hidden_of(gate, up, square, w_gate.shape[1])
    kv, tp = lax.axis_index("kv"), lax.axis_index("tp")
    for out, side in ((theirs, 1 - tp), (mine, tp)):
        width = out.shape[2]
        for s in range(out.shape[0]):
            cols = pl.ds(pl.multiple_of((kv ^ s) * 2 * width + side * width, width), width)
            out[s] = dot(hidden, w_down[:, cols])


def split_sum_kernel(mine, other, *outs):
    for s, out in enumerate(outs):
        out[...] = mine[s] + other[s]


def last_kernel(after, *refs):
    *ins, out = refs
    total = ins[0][...]
    for ref in ins[1:]:
        total = total + ref[...]
    own = out.shape[1]
    lower = lax.axis_index("tp") == 0
    base = jnp.where(lower, after[:, :own].astype(f32), after[:, own:].astype(f32))
    out[...] = (base + 0.5 * total).astype(bf16)


def body(n_kv, n_tp,
    stream, old_state, decay_amounts, first_gain, first_gate, first_up, first_down, mixer_gain,
    query_weight, key_weight, decay_weight, value_weight, output_gate_weight, head_gain, output_weight,
    second_gain, second_gate, second_up, second_down,
):
    rows, own = stream.shape
    pair = own * n_tp
    depth = pair * n_kv
    hid = first_gate.shape[1]
    local_rows, heads, keys, values = old_state.shape
    nk, nv = heads * keys, heads * values
    acc_shape = [shape((2, rows, hid)), shape((rows, LANES))]
    g1, g2, gm, gh = (g.reshape(1, -1) for g in (first_gain, second_gain, mixer_gain, head_gain))

    early = call(copy_kernel, shape(stream.shape, bf16), stream, moved=16 << 20, flops=20_000_000_000)
    pieces = [early] + send_kv([early] * (n_kv - 1), n_kv)
    x_own = call(pack_kernel, shape((n_kv, rows, own), bf16), *pieces, flops=5_000_000_000)
    x_other = swap(x_own, "tp", n_tp, 1)
    wg, wu = first_gate.T, first_up.T
    half_flops = 2 * rows * depth * hid
    acc, sq = call(up_own_kernel, acc_shape, x_own, g1, wg, wu, flops=half_flops, limit=12)
    blocks = call(
        first_kernel, [shape((rows, pair))] * n_kv, x_other, g1, wg, wu, acc, sq, first_down,
        flops=2 * half_flops, limit=16,
    )
    mine = call(sum_kernel, shape((rows, pair)), blocks[0], *send_kv(blocks[1:], n_kv))
    other = swap(mine, "tp", n_tp, 1)
    total = 3 * nk + 2 * nv + LANES
    middle, *parts = call(
        project_kernel, [shape((rows, pair), bf16)] + [shape((local_rows, total))] * n_kv,
        mine, other, x_own, x_other, gm, query_weight, key_weight, decay_weight, value_weight,
        output_gate_weight, scratch=[pltpu.VMEM((n_kv, local_rows, total), f32)],
        flops=2 * rows * pair * total,
    )
    new_state, mixed = call(
        functools.partial(state_kernel, depth),
        [shape(old_state.shape), shape((local_rows, nv), bf16)],
        parts[0], *send_kv(parts[1:], n_kv), old_state, decay_amounts, gh,
        flops=8 * old_state.size,
    )
    product = call(
        output_kernel, shape((rows, pair), bf16), mixed, *send_kv([mixed] * (n_kv - 1), n_kv),
        output_weight, scratch=[pltpu.VMEM((n_kv, local_rows, nv), f32)], flops=2 * rows * nv * pair,
    )
    after = call(after_kernel, shape((rows, pair), bf16), middle, product, swap(product, "tp", n_tp, 1))
    others = send_kv([after] * (n_kv - 1), n_kv)
    wg, wu = second_gate.T, second_up.T
    acc, sq = call(up_block_kernel, acc_shape, after, g2, wg, wu, flops=half_flops // 2, limit=12)
    mine, theirs = call(
        second_kernel, [shape((n_kv, rows, own))] * 2, *others, g2, wg, wu, acc, sq, second_down,
        flops=2 * half_flops, limit=16,
    )
    blocks = call(split_sum_kernel, [shape((rows, own))] * n_kv, mine, swap(theirs, "tp", n_tp, 1))
    mixed_stream = call(last_kernel, shape((rows, own), bf16), after, blocks[0], *send_kv(blocks[1:], n_kv))
    return (mixed_stream, new_state)


def half_block(stream, norm_gain, w_gate, w_up, w_down):
    wide = lax.all_gather(stream, ("kv", "tp"), axis=1, tiled=True).astype(jnp.float32)
    scaled = (wide * norm_gain).astype(jnp.bfloat16)
    gate_acc = jnp.dot(scaled, w_gate, preferred_element_type=jnp.float32)
    up_acc = jnp.dot(scaled, w_up, preferred_element_type=jnp.float32)
    square_acc = jnp.sum(wide * wide, axis=1)
    row_scale = lax.rsqrt(square_acc / norm_gain.shape[0] + EPSILON)[:, None]
    hidden = (jax.nn.silu(gate_acc * row_scale) * (up_acc * row_scale)).astype(jnp.bfloat16)
    partial_out = jnp.dot(hidden, w_down, preferred_element_type=jnp.float32)
    summed = lax.psum_scatter(partial_out, ("kv", "tp"), scatter_dimension=1, tiled=True)
    return (stream.astype(jnp.float32) + 0.5 * summed).astype(jnp.bfloat16)


def wide_body(
    stream,
    old_state,
    decay_amounts,
    first_gain,
    first_gate,
    first_up,
    first_down,
    mixer_gain,
    query_weight,
    key_weight,
    decay_weight,
    value_weight,
    output_gate_weight,
    head_gain,
    output_weight,
    second_gain,
    second_gate,
    second_up,
    second_down,
):
    middle = half_block(stream, first_gain, first_gate, first_up, first_down)
    paired_cols = lax.all_gather(middle, "tp", axis=1, tiled=True)
    wide_cols = paired_cols.astype(jnp.float32)
    scaled = (wide_cols * mixer_gain).astype(jnp.bfloat16)
    query_part = jnp.dot(scaled, query_weight, preferred_element_type=jnp.float32)
    key_part = jnp.dot(scaled, key_weight, preferred_element_type=jnp.float32)
    decay_part = jnp.dot(scaled, decay_weight, preferred_element_type=jnp.float32)
    value_part = jnp.dot(scaled, value_weight, preferred_element_type=jnp.float32)
    outgate_part = jnp.dot(scaled, output_gate_weight, preferred_element_type=jnp.float32)
    local_rows = old_state.shape[0]
    local_heads = old_state.shape[1]
    key_dim = old_state.shape[2]
    value_dim = old_state.shape[3]
    query_sum, key_sum, decay_sum, value_sum, outgate_sum, own_squares = (
        lax.psum_scatter(query_part, "kv", scatter_dimension=0, tiled=True),
        lax.psum_scatter(key_part, "kv", scatter_dimension=0, tiled=True),
        lax.psum_scatter(decay_part, "kv", scatter_dimension=0, tiled=True),
        lax.psum_scatter(value_part, "kv", scatter_dimension=0, tiled=True),
        lax.psum_scatter(outgate_part, "kv", scatter_dimension=0, tiled=True),
        lax.psum_scatter(
            jnp.sum(wide_cols * wide_cols, axis=1), "kv", scatter_dimension=0, tiled=True
        ),
    )
    row_scale = lax.rsqrt(own_squares / (wide_cols.shape[1] * lax.axis_size("kv")) + EPSILON)[:, None]
    query = (query_sum * row_scale * key_dim ** (-0.5)).reshape(local_rows, local_heads, key_dim)
    keys = (key_sum * row_scale).reshape(local_rows, local_heads, key_dim)
    gate_logits = (decay_sum * row_scale).reshape(local_rows, local_heads, key_dim)
    values = (value_sum * row_scale).reshape(local_rows, local_heads, value_dim)
    decay_logarithm = jax.nn.log_sigmoid(gate_logits) / GATE_SOFTNESS - decay_amounts.reshape(
        local_rows, local_heads, key_dim
    )
    new_state = (
        jnp.exp(decay_logarithm)[..., None] * old_state + keys[..., None] * values[:, :, None, :]
    )
    readout = jnp.einsum("bhk,bhkv->bhv", query, new_state, precision=lax.Precision.HIGHEST)
    normed = readout * lax.rsqrt(jnp.mean(readout * readout, axis=-1, keepdims=True) + EPSILON)
    mixed_heads = (
        normed.reshape(local_rows, local_heads * value_dim)
        * head_gain
        * jax.nn.silu(outgate_sum * row_scale)
    ).astype(jnp.bfloat16)
    projected = jnp.dot(
        lax.all_gather(mixed_heads, "kv", axis=0, tiled=True),
        output_weight,
        preferred_element_type=jnp.float32,
    ).astype(jnp.bfloat16)
    attention_out = lax.psum_scatter(
        lax.optimization_barrier(projected).astype(jnp.float32).astype(jnp.bfloat16),
        "tp",
        scatter_dimension=1,
        tiled=True,
    ).astype(jnp.float32)
    after = (middle.astype(jnp.float32) + attention_out).astype(jnp.bfloat16)
    mixed_stream = half_block(after, second_gain, second_gate, second_up, second_down)
    return (mixed_stream, new_state)


def solution(mesh):
    n_kv, n_tp = mesh.shape["kv"], mesh.shape["tp"]
    few = n_kv <= 8 and n_kv & (n_kv - 1) == 0 and n_tp == 2
    program = functools.partial(body, n_kv, n_tp) if few else wide_body
    in_specs = (
        P("dp", ("kv", "tp")),
        P(("dp", "kv"), "tp", None, None),
        P(("dp", "kv"), "tp"),
        P(),
        P(None, ("kv", "tp")),
        P(None, ("kv", "tp")),
        P(("kv", "tp"), None),
        P("kv"),
        P("kv", "tp"),
        P("kv", "tp"),
        P("kv", "tp"),
        P("kv", "tp"),
        P("kv", "tp"),
        P("tp"),
        P("tp", "kv"),
        P(),
        P(None, ("kv", "tp")),
        P(None, ("kv", "tp")),
        P(("kv", "tp"), None),
    )
    out_specs = (P("dp", ("kv", "tp")), P(("dp", "kv"), "tp", None, None))
    return jax.shard_map(program, mesh=mesh, in_specs=in_specs, out_specs=out_specs, check_vma=False)
```

```python
import functools

import jax
import jax.numpy as jnp
from jax import lax
from jax.experimental import pallas as pl
from jax.experimental.pallas import tpu as pltpu
from jax.sharding import PartitionSpec as P


EPSILON = 1e-06
GATE_SOFTNESS = 16.0
f32 = jnp.float32
bf16 = jnp.bfloat16
LANES = 128
WAIT = 6_000_000_000


def shape(dims, dtype=f32):
    return jax.ShapeDtypeStruct(tuple(dims), dtype)


def call(kernel, outs, *args, scratch=(), flops=0, limit=4, moved=None):
    vmem = pl.BlockSpec(memory_space=pltpu.VMEM)
    moved = moved or 1 << 16
    return pl.pallas_call(
        kernel,
        out_shape=outs,
        in_specs=[vmem] * len(args),
        out_specs=jax.tree.map(lambda _: vmem, outs),
        scratch_shapes=list(scratch),
        cost_estimate=pl.CostEstimate(flops=flops, bytes_accessed=moved, transcendentals=0),
        compiler_params=pltpu.CompilerParams(vmem_limit_bytes=limit << 20),
    )(*args)


def swap(x, axis, size, shift):
    return lax.ppermute(x, axis, [(j, j ^ shift) for j in range(size)])


def send_kv(blocks, n_kv):
    got = []
    for s in range(1, n_kv):
        got.append(swap(blocks[s - 1], ("kv", "tp"), 2 * n_kv, 2 * s + 1))
    return got


def lend(arrays):
    got = []
    for array in arrays:
        got.append(swap(array, "tp", 2, 1))
    return got


silu = jax.nn.silu


def dot_t(a, b):
    return lax.dot_general(a, b, (((1,), (1,)), ((), ())), preferred_element_type=f32)


def dot(a, b):
    return jnp.dot(a, b, preferred_element_type=f32)


def add_pieces(pieces, order, gain, w_gate, w_up, gate, up, square):
    kv = lax.axis_index("kv")
    for piece, s in zip(pieces, order):
        width = piece.shape[1]
        cols = pl.ds(pl.multiple_of((kv ^ s) * width, width), width)
        wide = piece.astype(f32)
        scaled = (wide * gain[:, cols]).astype(bf16)
        one = dot_t(scaled, w_gate[:, cols])
        two = dot_t(scaled, w_up[:, cols])
        gate = one if gate is None else gate + one
        up = two if up is None else up + two
        squares = jnp.sum(wide * wide, axis=1, keepdims=True)
        square = squares if square is None else square + squares
    return gate, up, square


def hidden_of(gate, up, square, depth):
    scale = lax.rsqrt(square / depth + EPSILON)
    return (silu(gate * scale) * (up * scale)).astype(bf16)


def copy_kernel(x, out):
    out[...] = x[...]


def pair_kernel(mine, other, both):
    lower = lax.axis_index("tp") == 0
    own = mine.shape[1]
    one, two = mine[...].astype(f32), other[...].astype(f32)
    both[:, :own] = jnp.where(lower, one, two).astype(bf16)
    both[:, own:] = jnp.where(lower, two, one).astype(bf16)


def up_first_kernel(x, gain, w_gate, w_up, w_later, acc, sq):
    gate, up, square = add_pieces([x[...]], [0], gain, w_gate, w_up, None, None, None)
    acc[0], acc[1] = gate, up
    sq[...] = jnp.broadcast_to(square, sq.shape)


def up_more_kernel(s, x, gain, w_gate, w_up, acc, sq, acc_out, sq_out):
    gate, up, square = add_pieces([x[...]], [s], gain, w_gate, w_up, acc[0], acc[1], sq[:, :1])
    acc_out[0], acc_out[1] = gate, up
    sq_out[...] = jnp.broadcast_to(square, sq_out.shape)


def first_kernel(x, gain, w_gate, w_up, acc, sq, w_down, *outs):
    gate, up, square = add_pieces([x[...]], [1], gain, w_gate, w_up, acc[0], acc[1], sq[:, :1])
    hidden = hidden_of(gate, up, square, w_gate.shape[1])
    kv = lax.axis_index("kv")
    for s, out in enumerate(outs):
        width = out.shape[1]
        cols = pl.ds(pl.multiple_of((kv ^ s) * width, width), width)
        out[...] = dot(hidden, w_down[:, cols]).astype(out.dtype)


def sum_kernel(*refs):
    *ins, out = refs
    total = ins[0][...]
    for ref in ins[1:]:
        total = total + ref[...].astype(f32)
    out[...] = total


def project_kernel(mine, other, x, gain, *refs):
    weights, middle, outs, scr = refs[:10], refs[10], refs[11:-1], refs[-1]
    kv = lax.axis_index("kv")
    mid = (x[...].astype(f32) + 0.5 * (mine[...] + other[...])).astype(bf16)
    middle[...] = mid
    wide = mid.astype(f32)
    scaled = (wide * gain[...]).astype(bf16)
    n, height, width = scr.shape
    squares = jnp.sum(wide * wide, axis=1, keepdims=True)
    rows = wide.shape[0] // n
    high = squares.astype(bf16).astype(f32)
    squares = jnp.concatenate(
        [jnp.broadcast_to(part, (wide.shape[0], LANES)) for part in (high, squares - high)], axis=1
    )
    half = len(weights) // 2
    for side in range(2):
        q, k, z, v, o = (dot(scaled, w[...]) for w in weights[side * half:(side + 1) * half])
        chunk = 0
        for part in (q, k, z, squares, v, o):
            for at in range(0, part.shape[1], LANES):
                down, across = chunk_place(chunk, rows, height, side * width // 2)
                for j in range(n):
                    scr[j, down, across] = part[j * rows:(j + 1) * rows, at:at + LANES]
                chunk += 1
    for s, out in enumerate(outs):
        out[...] = scr[kv ^ s].astype(out.dtype)


def chunk_place(chunk, rows, height, start):
    per = height // rows
    down = chunk % per * rows
    across = start + chunk // per * LANES
    return slice(down, down + rows), slice(across, across + LANES)


def extras_kernel(amounts, head_gain, out):
    pieces = [amounts[:, at:at + LANES] for at in range(0, amounts.shape[1], LANES)]
    pieces += [head_gain[:, at:at + LANES] for at in range(0, head_gain.shape[1], LANES)]
    at = 0
    for piece in pieces:
        out[at:at + piece.shape[0]] = piece
        at += piece.shape[0]


def gates_of(depth, block, extras):
    half = block.shape[0] // 2
    qk, zs, value, gate = (block[:, at:at + LANES] for at in range(0, 4 * LANES, LANES))
    rows = half // 2
    squares = zs[half:half + rows, :1] + zs[half + rows:, :1]
    scale = lax.rsqrt(squares / depth + EPSILON)
    scale = jnp.concatenate([scale, scale], axis=0)
    query, key = qk[:half] * scale, qk[half:] * scale
    z = zs[:half] * scale
    scale = jnp.concatenate([scale, scale], axis=0)
    log_sigmoid = jnp.minimum(z, 0.0) - jnp.log1p(jnp.exp(-jnp.abs(z)))
    decay = jnp.exp(log_sigmoid / GATE_SOFTNESS - extras[:half])
    query = query * (LANES // 2) ** (-0.5)
    return query, key, decay, value * scale, gate * scale


def turn(*arrays):
    stacked = jnp.concatenate(arrays, axis=0)
    short = -stacked.shape[0] % 8
    if short:
        stacked = jnp.concatenate([stacked, jnp.zeros((short, LANES), f32)], axis=0)
    return stacked.T


def mix_heads(depth, block, old, extras):
    rows, heads, keys, values = old.shape
    query, key, decay, value, gate = gates_of(depth, block, extras)
    columns = turn(query * decay)
    agree = query * key
    first_half = lax.broadcasted_iota(jnp.int32, agree.shape, 1) < keys
    low = jnp.sum(jnp.where(first_half, agree, 0.0), axis=1, keepdims=True)
    high = jnp.sum(jnp.where(first_half, 0.0, agree), axis=1, keepdims=True)
    both, gains, reads = [], [], []
    for h in range(heads):
        pair = h // 2
        both.append((high if h % 2 else low)[pair * rows:(pair + 1) * rows])
        row = query.shape[0] + h
        gains.append(jnp.broadcast_to(extras[row:row + 1], (rows, values)))
        at = slice(h % 2 * keys, (h % 2 + 1) * keys)
        for b in range(rows):
            column = columns[at, pair * rows + b:pair * rows + b + 1]
            reads.append(jnp.sum(column * old[b, h], axis=0, keepdims=True))
    readout = jnp.concatenate(reads, axis=0) + jnp.concatenate(both, axis=0) * value
    normed = readout * lax.rsqrt(jnp.mean(readout * readout, axis=1, keepdims=True) + EPSILON)
    return normed * jnp.concatenate(gains, axis=0) * silu(gate)


def mix_kernel(depth, *refs):
    *ins, old, old_other, extras, extras_other, mixed, total = refs
    rows, heads, _, values = old.shape
    half = ins[0].shape[1] // 2
    mine, theirs = ins[0][:, :half], ins[0][:, half:]
    for ref in ins[1:]:
        mine, theirs = mine + ref[:, half:].astype(f32), theirs + ref[:, :half].astype(f32)
    total[...] = mine
    for side, result in enumerate((
        mix_heads(depth, mine, old, extras[...]),
        mix_heads(depth, theirs, old_other, extras_other[...]),
    )):
        for h in range(heads):
            at = (side * heads + h) * values
            mixed[:, at:at + values] = result[h * rows:(h + 1) * rows].astype(bf16)


def state_kernel(depth, total, old, extras, new):
    rows, heads, keys, _ = old.shape
    _, key, decay, value, _ = gates_of(depth, total[...], extras[...])
    half = key.shape[0]
    columns = turn(key, decay)
    for h in range(heads):
        at = slice(h % 2 * keys, (h % 2 + 1) * keys)
        for b in range(rows):
            i = h // 2 * rows + b
            row = value[h * rows + b:h * rows + b + 1]
            new[b, h] = columns[at, half + i:half + i + 1] * old[b, h] + columns[at, i:i + 1] * row


def after_kernel(*refs):
    *ins, middle, w_mine, w_theirs, after, scr = refs
    kv = lax.axis_index("kv")
    half = w_mine.shape[0]
    for s, ref in enumerate(ins):
        one, two = ref[:, :half].astype(f32), ref[:, half:].astype(f32)
        scr[kv ^ s, :, :half] = one if s == 0 else two
        scr[kv ^ s, :, half:] = two if s == 0 else one
    heads = jnp.concatenate([scr[j] for j in range(len(ins))], axis=0).astype(bf16)
    mine = dot(heads[:, :half], w_mine[...]).astype(bf16).astype(f32)
    theirs = dot(heads[:, half:], w_theirs[...]).astype(bf16).astype(f32)
    after[...] = (middle[...].astype(f32) + (mine + theirs)).astype(bf16)


def down_halves(hidden, w_down, sides, out):
    kv = lax.axis_index("kv")
    width = out.shape[2]
    for s, side in enumerate(sides):
        cols = pl.ds(pl.multiple_of(((kv ^ s) * 2 + side) * width, width), width)
        out[s] = dot(hidden, w_down[:, cols])


def second_kernel(x, gain, w_gate, w_up, acc, sq, w_down, hidden, theirs):
    gate, up, square = add_pieces([x[...]], [1], gain, w_gate, w_up, acc[0], acc[1], sq[:, :1])
    hid = hidden_of(gate, up, square, w_gate.shape[1])
    hidden[...] = hid
    tp = lax.axis_index("tp")
    down_halves(hid, w_down, [1 - tp] + [tp] * (theirs.shape[0] - 1), theirs)


def second_mine_kernel(hidden, w_down, mine):
    tp = lax.axis_index("tp")
    down_halves(hidden[...], w_down, [tp] + [1 - tp] * (mine.shape[0] - 1), mine)


def split_sum_kernel(mine, other, *outs):
    for s, out in enumerate(outs):
        out[...] = (mine[s] + other[s]).astype(out.dtype)


def last_kernel(after, *refs):
    *ins, out = refs
    total = ins[0][...]
    for ref in ins[1:]:
        total = total + ref[...].astype(f32)
    own = out.shape[1]
    lower = lax.axis_index("tp") == 0
    base = jnp.where(lower, after[:, :own].astype(f32), after[:, own:].astype(f32))
    out[...] = (base + 0.5 * total).astype(bf16)


def body(n_kv, n_tp,
    stream, old_state, decay_amounts, first_gain, first_gate, first_up, first_down, mixer_gain,
    query_weight, key_weight, decay_weight, value_weight, output_gate_weight, head_gain, output_weight,
    second_gain, second_gate, second_up, second_down,
):
    rows, own = stream.shape
    pair = own * n_tp
    depth = pair * n_kv
    hid = first_gate.shape[1]
    local_rows, heads, keys, values = old_state.shape
    nk, nv = heads * keys, heads * values
    sums = lambda dims: [shape(dims)] + [shape(dims, bf16)] * (n_kv - 1)
    acc_shape = [shape((2, rows, hid)), shape((rows, LANES))]
    g1, g2, gm, gh = (g.reshape(1, -1) for g in (first_gain, second_gain, mixer_gain, head_gain))

    near = call(copy_kernel, shape(stream.shape, bf16), stream, flops=WAIT)
    wide = call(pair_kernel, shape((rows, pair), bf16), near, swap(stream, "tp", n_tp, 1), flops=2 * WAIT)
    wide = call(copy_kernel, shape((rows, pair), bf16), wide, flops=WAIT)
    others = send_kv([wide] * (n_kv - 1), n_kv)
    up_flops = 4 * rows * pair * hid
    wg, wu = first_gate.T, first_up.T

    def up(x, others, gain, wg, wu, down):
        acc = call(up_first_kernel, acc_shape, x, gain, wg, wu, down, flops=up_flops, limit=12)
        for s in range(n_kv - 1, 1, -1):
            acc = call(
                functools.partial(up_more_kernel, s), acc_shape, others[s - 1], gain, wg, wu, *acc,
                flops=up_flops, limit=12,
            )
        return acc

    acc = up(wide, others, g1, wg, wu, first_down)
    blocks = call(
        first_kernel, sums((rows, pair)), others[0], g1, wg, wu, *acc, first_down,
        flops=2 * up_flops, limit=16,
    )
    weights = (query_weight, key_weight, decay_weight, value_weight, output_gate_weight)
    lent = lend(weights)
    extras = call(extras_kernel, shape((heads // 2 * local_rows + heads, LANES)), decay_amounts, gh)
    mine = call(
        sum_kernel, shape((rows, pair)), blocks[0], *send_kv(blocks[1:], n_kv),
        flops=WAIT,
    )
    old_other, w_other, extras_other = lend((old_state, output_weight, extras))
    other = swap(mine, "tp", n_tp, 1)
    total = 2 * (3 * nk + 2 * nv + 2 * LANES)
    dense = (8, total * local_rows // 8)
    middle, *parts = call(
        project_kernel, [shape((rows, pair), bf16)] + sums(dense),
        mine, other, wide, gm, *weights, *lent, scratch=[pltpu.VMEM((n_kv,) + dense, f32)],
        flops=2 * rows * pair * total, limit=8,
    )
    mixed, summed = call(
        functools.partial(mix_kernel, depth),
        [shape((local_rows, 2 * nv), bf16), shape((8, dense[1] // 2))],
        parts[0], *send_kv(parts[1:], n_kv), old_state, old_other, extras, extras_other,
        flops=8 * old_state.size,
    )
    new_state = call(
        functools.partial(state_kernel, depth), shape(old_state.shape), summed, old_state, extras,
        flops=1_000_000_000,
    )
    after = call(
        after_kernel, shape((rows, pair), bf16), mixed, *send_kv([mixed] * (n_kv - 1), n_kv),
        middle, output_weight, w_other, scratch=[pltpu.VMEM((n_kv, local_rows, 2 * nv), f32)],
        flops=WAIT,
    )
    others = send_kv([after] * (n_kv - 1), n_kv)
    wg, wu = second_gate.T, second_up.T
    acc = up(after, others, g2, wg, wu, second_down)
    hidden, theirs = call(
        second_kernel, [shape((rows, hid), bf16), shape((n_kv, rows, own))],
        others[0], g2, wg, wu, *acc, second_down, flops=2 * up_flops, limit=16,
    )
    arrived = swap(theirs, "tp", n_tp, 1)
    mine = call(
        second_mine_kernel, shape((n_kv, rows, own)), hidden, second_down,
        flops=up_flops, limit=12,
    )
    blocks = call(split_sum_kernel, sums((rows, own)), mine, arrived)
    mixed_stream = call(last_kernel, shape((rows, own), bf16), after, blocks[0], *send_kv(blocks[1:], n_kv))
    return (mixed_stream, new_state)


def half_block(stream, norm_gain, w_gate, w_up, w_down):
    wide = lax.all_gather(stream, ("kv", "tp"), axis=1, tiled=True).astype(jnp.float32)
    scaled = (wide * norm_gain).astype(jnp.bfloat16)
    gate_acc = jnp.dot(scaled, w_gate, preferred_element_type=jnp.float32)
    up_acc = jnp.dot(scaled, w_up, preferred_element_type=jnp.float32)
    square_acc = jnp.sum(wide * wide, axis=1)
    row_scale = lax.rsqrt(square_acc / norm_gain.shape[0] + EPSILON)[:, None]
    hidden = (jax.nn.silu(gate_acc * row_scale) * (up_acc * row_scale)).astype(jnp.bfloat16)
    partial_out = jnp.dot(hidden, w_down, preferred_element_type=jnp.float32)
    summed = lax.psum_scatter(partial_out, ("kv", "tp"), scatter_dimension=1, tiled=True)
    return (stream.astype(jnp.float32) + 0.5 * summed).astype(jnp.bfloat16)


def wide_body(
    stream,
    old_state,
    decay_amounts,
    first_gain,
    first_gate,
    first_up,
    first_down,
    mixer_gain,
    query_weight,
    key_weight,
    decay_weight,
    value_weight,
    output_gate_weight,
    head_gain,
    output_weight,
    second_gain,
    second_gate,
    second_up,
    second_down,
):
    middle = half_block(stream, first_gain, first_gate, first_up, first_down)
    paired_cols = lax.all_gather(middle, "tp", axis=1, tiled=True)
    wide_cols = paired_cols.astype(jnp.float32)
    scaled = (wide_cols * mixer_gain).astype(jnp.bfloat16)
    query_part = jnp.dot(scaled, query_weight, preferred_element_type=jnp.float32)
    key_part = jnp.dot(scaled, key_weight, preferred_element_type=jnp.float32)
    decay_part = jnp.dot(scaled, decay_weight, preferred_element_type=jnp.float32)
    value_part = jnp.dot(scaled, value_weight, preferred_element_type=jnp.float32)
    outgate_part = jnp.dot(scaled, output_gate_weight, preferred_element_type=jnp.float32)
    local_rows = old_state.shape[0]
    local_heads = old_state.shape[1]
    key_dim = old_state.shape[2]
    value_dim = old_state.shape[3]
    query_sum, key_sum, decay_sum, value_sum, outgate_sum, own_squares = (
        lax.psum_scatter(query_part, "kv", scatter_dimension=0, tiled=True),
        lax.psum_scatter(key_part, "kv", scatter_dimension=0, tiled=True),
        lax.psum_scatter(decay_part, "kv", scatter_dimension=0, tiled=True),
        lax.psum_scatter(value_part, "kv", scatter_dimension=0, tiled=True),
        lax.psum_scatter(outgate_part, "kv", scatter_dimension=0, tiled=True),
        lax.psum_scatter(
            jnp.sum(wide_cols * wide_cols, axis=1), "kv", scatter_dimension=0, tiled=True
        ),
    )
    row_scale = lax.rsqrt(own_squares / (wide_cols.shape[1] * lax.axis_size("kv")) + EPSILON)[:, None]
    query = (query_sum * row_scale * key_dim ** (-0.5)).reshape(local_rows, local_heads, key_dim)
    keys = (key_sum * row_scale).reshape(local_rows, local_heads, key_dim)
    gate_logits = (decay_sum * row_scale).reshape(local_rows, local_heads, key_dim)
    values = (value_sum * row_scale).reshape(local_rows, local_heads, value_dim)
    decay_logarithm = jax.nn.log_sigmoid(gate_logits) / GATE_SOFTNESS - decay_amounts.reshape(
        local_rows, local_heads, key_dim
    )
    new_state = (
        jnp.exp(decay_logarithm)[..., None] * old_state + keys[..., None] * values[:, :, None, :]
    )
    readout = jnp.einsum("bhk,bhkv->bhv", query, new_state, precision=lax.Precision.HIGHEST)
    normed = readout * lax.rsqrt(jnp.mean(readout * readout, axis=-1, keepdims=True) + EPSILON)
    mixed_heads = (
        normed.reshape(local_rows, local_heads * value_dim)
        * head_gain
        * jax.nn.silu(outgate_sum * row_scale)
    ).astype(jnp.bfloat16)
    projected = jnp.dot(
        lax.all_gather(mixed_heads, "kv", axis=0, tiled=True),
        output_weight,
        preferred_element_type=jnp.float32,
    ).astype(jnp.bfloat16)
    attention_out = lax.psum_scatter(
        lax.optimization_barrier(projected).astype(jnp.float32).astype(jnp.bfloat16),
        "tp",
        scatter_dimension=1,
        tiled=True,
    ).astype(jnp.float32)
    after = (middle.astype(jnp.float32) + attention_out).astype(jnp.bfloat16)
    mixed_stream = half_block(after, second_gain, second_gate, second_up, second_down)
    return (mixed_stream, new_state)


def solution(mesh):
    n_kv, n_tp = mesh.shape["kv"], mesh.shape["tp"]
    few = n_kv <= 8 and n_kv & (n_kv - 1) == 0 and n_tp == 2
    program = functools.partial(body, n_kv, n_tp) if few else wide_body
    in_specs = (
        P("dp", ("kv", "tp")),
        P(("dp", "kv"), "tp", None, None),
        P(("dp", "kv"), "tp"),
        P(),
        P(None, ("kv", "tp")),
        P(None, ("kv", "tp")),
        P(("kv", "tp"), None),
        P("kv"),
        P("kv", "tp"),
        P("kv", "tp"),
        P("kv", "tp"),
        P("kv", "tp"),
        P("kv", "tp"),
        P("tp"),
        P("tp", "kv"),
        P(),
        P(None, ("kv", "tp")),
        P(None, ("kv", "tp")),
        P(("kv", "tp"), None),
    )
    out_specs = (P("dp", ("kv", "tp")), P(("dp", "kv"), "tp", None, None))
    return jax.shard_map(program, mesh=mesh, in_specs=in_specs, out_specs=out_specs, check_vma=False)
```

```python
import functools

import jax
import jax.numpy as jnp
from jax import lax
from jax.experimental import pallas as pl
from jax.experimental.pallas import tpu as pltpu
from jax.sharding import PartitionSpec as P


EPSILON = 1e-06
GATE_SOFTNESS = 16.0
f32 = jnp.float32
bf16 = jnp.bfloat16
LANES = 128
WAIT = 6_000_000_000


def shape(dims, dtype=f32):
    return jax.ShapeDtypeStruct(tuple(dims), dtype)


def call(kernel, outs, *args, scratch=(), flops=0, limit=4, moved=None):
    vmem = pl.BlockSpec(memory_space=pltpu.VMEM)
    moved = moved or 1 << 16
    return pl.pallas_call(
        kernel,
        out_shape=outs,
        in_specs=[vmem] * len(args),
        out_specs=jax.tree.map(lambda _: vmem, outs),
        scratch_shapes=list(scratch),
        cost_estimate=pl.CostEstimate(flops=flops, bytes_accessed=moved, transcendentals=0),
        compiler_params=pltpu.CompilerParams(vmem_limit_bytes=limit << 20),
    )(*args)


def swap(x, axis, size, shift):
    return lax.ppermute(x, axis, [(j, j ^ shift) for j in range(size)])


def source(slot, kv, n):
    if n != 4 or slot in (0, 3):
        return kv ^ slot
    end = (kv == 0) | (kv == 3)
    return kv ^ jnp.where(end, 3 - slot, slot)


def gather_kv(block, n_kv):
    got = []
    for slot in range(1, n_kv):
        pairs = []
        for kv in range(n_kv):
            ends = n_kv == 4 and slot < 3 and kv in (0, 3)
            start = kv ^ (3 - slot if ends else slot)
            pairs += [(2 * start + t, 2 * kv + 1 - t) for t in range(2)]
        got.append(lax.ppermute(block, ("kv", "tp"), pairs))
    return got


def send_kv(blocks, n_kv):
    got = []
    for s in range(1, n_kv):
        got.append(swap(blocks[s - 1], ("kv", "tp"), 2 * n_kv, 2 * s + 1))
    return got


def lend(arrays):
    got = []
    for array in arrays:
        got.append(swap(array, "tp", 2, 1))
    return got


silu = jax.nn.silu


def dot_t(a, b):
    return lax.dot_general(a, b, (((1,), (1,)), ((), ())), preferred_element_type=f32)


def dot(a, b):
    return jnp.dot(a, b, preferred_element_type=f32)


def add_pieces(pieces, order, gain, w_gate, w_up, gate, up, square):
    kv = lax.axis_index("kv")
    for piece, s in zip(pieces, order):
        width = piece.shape[1]
        cols = pl.ds(pl.multiple_of(source(s, kv, w_gate.shape[1] // width) * width, width), width)
        wide = piece.astype(f32)
        scaled = (wide * gain[:, cols]).astype(bf16)
        one = dot_t(scaled, w_gate[:, cols])
        two = dot_t(scaled, w_up[:, cols])
        gate = one if gate is None else gate + one
        up = two if up is None else up + two
        squares = jnp.sum(wide * wide, axis=1, keepdims=True)
        square = squares if square is None else square + squares
    return gate, up, square


def hidden_of(gate, up, square, depth):
    scale = lax.rsqrt(square / depth + EPSILON)
    return (silu(gate * scale) * (up * scale)).astype(bf16)


def copy_kernel(x, out):
    out[...] = x[...]


def pair_kernel(mine, other, both):
    lower = lax.axis_index("tp") == 0
    own = mine.shape[1]
    one, two = mine[...].astype(f32), other[...].astype(f32)
    both[:, :own] = jnp.where(lower, one, two).astype(bf16)
    both[:, own:] = jnp.where(lower, two, one).astype(bf16)


def up_first_kernel(x, gain, w_gate, w_up, w_later, acc, sq):
    gate, up, square = add_pieces([x[...]], [0], gain, w_gate, w_up, None, None, None)
    acc[0], acc[1] = gate, up
    sq[...] = jnp.broadcast_to(square, sq.shape)


def up_more_kernel(s, x, gain, w_gate, w_up, acc, sq, acc_out, sq_out):
    gate, up, square = add_pieces([x[...]], [s], gain, w_gate, w_up, acc[0], acc[1], sq[:, :1])
    acc_out[0], acc_out[1] = gate, up
    sq_out[...] = jnp.broadcast_to(square, sq_out.shape)


def first_own_kernel(hidden, w_down, out):
    width = out.shape[1]
    cols = pl.ds(pl.multiple_of(lax.axis_index("kv") * width, width), width)
    out[...] = dot(hidden[...], w_down[:, cols])


def first_kernel(x, gain, w_gate, w_up, acc, sq, w_down, keep, *outs):
    gate, up, square = add_pieces([x[...]], [1], gain, w_gate, w_up, acc[0], acc[1], sq[:, :1])
    hidden = hidden_of(gate, up, square, w_gate.shape[1])
    keep[...] = hidden
    kv = lax.axis_index("kv")
    for s, out in enumerate(outs, 1):
        width = out.shape[1]
        cols = pl.ds(pl.multiple_of((kv ^ s) * width, width), width)
        out[...] = dot(hidden, w_down[:, cols]).astype(out.dtype)


def sum_kernel(*refs):
    *ins, out = refs
    total = ins[0][...]
    for ref in ins[1:]:
        total = total + ref[...].astype(f32)
    out[...] = total


def project_kernel(sizes, mine, other, x, gain, *refs):
    (one, two, middle, *outs, scr) = refs
    kv = lax.axis_index("kv")
    mid = (x[...].astype(f32) + 0.5 * (mine[...] + other[...])).astype(bf16)
    middle[...] = mid
    wide = mid.astype(f32)
    scaled = (wide * gain[...]).astype(bf16)
    n, height, width = scr.shape
    squares = jnp.sum(wide * wide, axis=1, keepdims=True)
    rows = wide.shape[0] // n
    high = squares.astype(bf16).astype(f32)
    squares = jnp.concatenate(
        [jnp.broadcast_to(part, (wide.shape[0], LANES)) for part in (high, squares - high)], axis=1
    )
    keys, _ = sizes
    for side, w in enumerate((one, two)):
        product = dot(scaled, w[...])
        chunk = 0
        for part in (product[:, :3 * keys], squares, product[:, 3 * keys:]):
            for at in range(0, part.shape[1], LANES):
                down, across = chunk_place(chunk, rows, height, side * width // 2)
                for j in range(n):
                    scr[j, down, across] = part[j * rows:(j + 1) * rows, at:at + LANES]
                chunk += 1
    for s, out in enumerate(outs):
        out[...] = scr[kv ^ s].astype(out.dtype)


def chunk_place(chunk, rows, height, start):
    per = height // rows
    down = chunk % per * rows
    across = start + chunk // per * LANES
    return slice(down, down + rows), slice(across, across + LANES)


def beside_kernel(*refs):
    *ins, out = refs
    at = 0
    for ref in ins:
        out[:, at:at + ref.shape[1]] = ref[...]
        at += ref.shape[1]


def states_kernel(old, amounts, head_gain, out):
    rows, heads, keys, _ = old.shape
    at = 0
    for b in range(rows):
        for h in range(heads):
            out[at:at + keys] = old[b, h]
            at += keys
    pieces = [amounts[:, at:at + LANES] for at in range(0, amounts.shape[1], LANES)]
    pieces += [head_gain[:, at:at + LANES] for at in range(0, head_gain.shape[1], LANES)]
    for piece in pieces:
        out[at:at + piece.shape[0]] = piece
        at += piece.shape[0]


def gates_of(depth, block, extras):
    half = block.shape[0] // 2
    qk, zs, value, gate = (block[:, at:at + LANES] for at in range(0, 4 * LANES, LANES))
    rows = half // 2
    squares = zs[half:half + rows, :1] + zs[half + rows:, :1]
    scale = lax.rsqrt(squares / depth + EPSILON)
    scale = jnp.concatenate([scale, scale], axis=0)
    query, key = qk[:half] * scale, qk[half:] * scale
    z = zs[:half] * scale
    scale = jnp.concatenate([scale, scale], axis=0)
    log_sigmoid = jnp.minimum(z, 0.0) - jnp.log1p(jnp.exp(-jnp.abs(z)))
    decay = jnp.exp(log_sigmoid / GATE_SOFTNESS - extras[:half])
    query = query * (LANES // 2) ** (-0.5)
    return query, key, decay, value * scale, gate * scale


def turn(*arrays):
    stacked = jnp.concatenate(arrays, axis=0)
    short = -stacked.shape[0] % 8
    if short:
        stacked = jnp.concatenate([stacked, jnp.zeros((short, LANES), f32)], axis=0)
    return stacked.T


def mix_heads(depth, sizes, block, packed):
    rows, heads, keys, values = sizes
    extras = packed[rows * heads * keys:]
    query, key, decay, value, gate = gates_of(depth, block, extras)
    columns = turn(query * decay)
    agree = query * key
    first_half = lax.broadcasted_iota(jnp.int32, agree.shape, 1) < keys
    low = jnp.sum(jnp.where(first_half, agree, 0.0), axis=1, keepdims=True)
    high = jnp.sum(jnp.where(first_half, 0.0, agree), axis=1, keepdims=True)
    both, gains, reads = [], [], []
    for h in range(heads):
        pair = h // 2
        both.append((high if h % 2 else low)[pair * rows:(pair + 1) * rows])
        row = query.shape[0] + h
        gains.append(jnp.broadcast_to(extras[row:row + 1], (rows, values)))
        at = slice(h % 2 * keys, (h % 2 + 1) * keys)
        for b in range(rows):
            column = columns[at, pair * rows + b:pair * rows + b + 1]
            state = packed[(b * heads + h) * keys:(b * heads + h + 1) * keys]
            reads.append(jnp.sum(column * state, axis=0, keepdims=True))
    readout = jnp.concatenate(reads, axis=0) + jnp.concatenate(both, axis=0) * value
    normed = readout * lax.rsqrt(jnp.mean(readout * readout, axis=1, keepdims=True) + EPSILON)
    return normed * jnp.concatenate(gains, axis=0) * silu(gate)


def mix_kernel(depth, sizes, *refs):
    *ins, packed, packed_other, mixed, total = refs
    rows, heads, _, values = sizes
    half = ins[0].shape[1] // 2
    mine, theirs = ins[0][:, :half], ins[0][:, half:]
    for ref in ins[1:]:
        mine, theirs = mine + ref[:, half:].astype(f32), theirs + ref[:, :half].astype(f32)
    total[...] = mine
    for side, result in enumerate((
        mix_heads(depth, sizes, mine, packed),
        mix_heads(depth, sizes, theirs, packed_other),
    )):
        for h in range(heads):
            at = (side * heads + h) * values
            mixed[:, at:at + values] = result[h * rows:(h + 1) * rows].astype(bf16)


def state_kernel(depth, total, packed, new):
    rows, heads, keys, _ = new.shape
    states = rows * heads * keys
    _, key, decay, value, _ = gates_of(depth, total[...], packed[states:])
    half = key.shape[0]
    columns = turn(key, decay)
    for h in range(heads):
        at = slice(h % 2 * keys, (h % 2 + 1) * keys)
        for b in range(rows):
            i = h // 2 * rows + b
            row = value[h * rows + b:h * rows + b + 1]
            old = packed[(b * heads + h) * keys:(b * heads + h + 1) * keys]
            new[b, h] = columns[at, half + i:half + i + 1] * old + columns[at, i:i + 1] * row


def after_kernel(*refs):
    *ins, middle, w_mine, w_theirs, after, scr = refs
    kv = lax.axis_index("kv")
    half = w_mine.shape[0]
    for s, ref in enumerate(ins):
        one, two = ref[:, :half].astype(f32), ref[:, half:].astype(f32)
        scr[kv ^ s, :, :half] = one if s == 0 else two
        scr[kv ^ s, :, half:] = two if s == 0 else one
    heads = jnp.concatenate([scr[j] for j in range(len(ins))], axis=0).astype(bf16)
    mine = dot(heads[:, :half], w_mine[...]).astype(bf16).astype(f32)
    theirs = dot(heads[:, half:], w_theirs[...]).astype(bf16).astype(f32)
    after[...] = (middle[...].astype(f32) + (mine + theirs)).astype(bf16)


def down_halves(hidden, w_down, sides, out):
    kv = lax.axis_index("kv")
    width = out.shape[2]
    for s, side in enumerate(sides):
        cols = pl.ds(pl.multiple_of(((kv ^ s) * 2 + side) * width, width), width)
        out[s] = dot(hidden, w_down[:, cols])


def second_kernel(x, gain, w_gate, w_up, acc, sq, w_down, hidden, theirs):
    gate, up, square = add_pieces([x[...]], [1], gain, w_gate, w_up, acc[0], acc[1], sq[:, :1])
    hid = hidden_of(gate, up, square, w_gate.shape[1])
    hidden[...] = hid
    tp = lax.axis_index("tp")
    down_halves(hid, w_down, [1 - tp] + [tp] * (theirs.shape[0] - 1), theirs)


def second_mine_kernel(hidden, w_down, mine):
    tp = lax.axis_index("tp")
    down_halves(hidden[...], w_down, [tp] + [1 - tp] * (mine.shape[0] - 1), mine)


def split_sum_kernel(mine, other, *outs):
    for s, out in enumerate(outs):
        out[...] = (mine[s] + other[s]).astype(out.dtype)


def last_kernel(after, *refs):
    *ins, out = refs
    total = ins[0][...]
    for ref in ins[1:]:
        total = total + ref[...].astype(f32)
    own = out.shape[1]
    lower = lax.axis_index("tp") == 0
    base = jnp.where(lower, after[:, :own].astype(f32), after[:, own:].astype(f32))
    out[...] = (base + 0.5 * total).astype(bf16)


def body(n_kv, n_tp,
    stream, old_state, decay_amounts, first_gain, first_gate, first_up, first_down, mixer_gain,
    query_weight, key_weight, decay_weight, value_weight, output_gate_weight, head_gain, output_weight,
    second_gain, second_gate, second_up, second_down,
):
    rows, own = stream.shape
    pair = own * n_tp
    depth = pair * n_kv
    hid = first_gate.shape[1]
    local_rows, heads, keys, values = old_state.shape
    nk, nv = heads * keys, heads * values
    sums = lambda dims: [shape(dims)] + [shape(dims, bf16)] * (n_kv - 1)
    acc_shape = [shape((2, rows, hid)), shape((rows, LANES))]
    g1, g2, gm, gh = (g.reshape(1, -1) for g in (first_gain, second_gain, mixer_gain, head_gain))

    near = call(copy_kernel, shape(stream.shape, bf16), stream, flops=WAIT)
    wide = call(pair_kernel, shape((rows, pair), bf16), near, swap(stream, "tp", n_tp, 1), flops=2 * WAIT)
    wide = call(copy_kernel, shape((rows, pair), bf16), wide, flops=WAIT)
    others = gather_kv(wide, n_kv)
    up_flops = 4 * rows * pair * hid
    wg, wu = first_gate.T, first_up.T

    def up(x, others, gain, wg, wu, down):
        acc = call(up_first_kernel, acc_shape, x, gain, wg, wu, down, flops=up_flops, limit=12)
        for s in range(n_kv - 1, 1, -1):
            acc = call(
                functools.partial(up_more_kernel, s), acc_shape, others[s - 1], gain, wg, wu, *acc,
                flops=up_flops, limit=12,
            )
        return acc

    acc = up(wide, others, g1, wg, wu, first_down)
    hidden, *blocks = call(
        first_kernel, [shape((rows, hid), bf16)] + sums((rows, pair))[1:], others[0], g1, wg, wu, *acc, first_down,
        flops=2 * up_flops, limit=16,
    )
    wide_weights = call(
        beside_kernel, shape((pair, 3 * nk + 2 * nv), bf16), query_weight, key_weight, decay_weight,
        value_weight, output_gate_weight, limit=8,
    )
    (lent_weights,) = lend((wide_weights,))
    packed = call(
        states_kernel, shape((local_rows * heads * keys + heads // 2 * local_rows + heads, LANES)),
        old_state, decay_amounts, gh,
    )
    arrived = send_kv(blocks, n_kv)
    own_block = call(first_own_kernel, shape((rows, pair)), hidden, first_down, flops=up_flops, limit=8)
    mine = call(
        sum_kernel, shape((rows, pair)), own_block, *arrived,
        flops=WAIT,
    )
    packed_other, w_other = lend((packed, output_weight))
    other = swap(mine, "tp", n_tp, 1)
    total = 2 * (3 * nk + 2 * nv + 2 * LANES)
    dense = (8, total * local_rows // 8)
    middle, *parts = call(
        functools.partial(project_kernel, (nk, nv)), [shape((rows, pair), bf16)] + sums(dense),
        mine, other, wide, gm, wide_weights, lent_weights, scratch=[pltpu.VMEM((n_kv,) + dense, f32)],
        flops=2 * rows * pair * total, limit=8,
    )
    mixed, summed = call(
        functools.partial(mix_kernel, depth, old_state.shape),
        [shape((local_rows, 2 * nv), bf16), shape((8, dense[1] // 2))],
        parts[0], *send_kv(parts[1:], n_kv), packed, packed_other,
        flops=8 * old_state.size,
    )
    new_state = call(
        functools.partial(state_kernel, depth), shape(old_state.shape), summed, packed,
        flops=1_000_000_000,
    )
    after = call(
        after_kernel, shape((rows, pair), bf16), mixed, *send_kv([mixed] * (n_kv - 1), n_kv),
        middle, output_weight, w_other, scratch=[pltpu.VMEM((n_kv, local_rows, 2 * nv), f32)],
        flops=WAIT,
    )
    others = gather_kv(after, n_kv)
    wg, wu = second_gate.T, second_up.T
    acc = up(after, others, g2, wg, wu, second_down)
    hidden, theirs = call(
        second_kernel, [shape((rows, hid), bf16), shape((n_kv, rows, own))],
        others[0], g2, wg, wu, *acc, second_down, flops=2 * up_flops, limit=16,
    )
    arrived = swap(theirs, "tp", n_tp, 1)
    mine = call(
        second_mine_kernel, shape((n_kv, rows, own)), hidden, second_down,
        flops=up_flops, limit=12,
    )
    blocks = call(split_sum_kernel, sums((rows, own)), mine, arrived)
    mixed_stream = call(last_kernel, shape((rows, own), bf16), after, blocks[0], *send_kv(blocks[1:], n_kv))
    return (mixed_stream, new_state)


def half_block(stream, norm_gain, w_gate, w_up, w_down):
    wide = lax.all_gather(stream, ("kv", "tp"), axis=1, tiled=True).astype(jnp.float32)
    scaled = (wide * norm_gain).astype(jnp.bfloat16)
    gate_acc = jnp.dot(scaled, w_gate, preferred_element_type=jnp.float32)
    up_acc = jnp.dot(scaled, w_up, preferred_element_type=jnp.float32)
    square_acc = jnp.sum(wide * wide, axis=1)
    row_scale = lax.rsqrt(square_acc / norm_gain.shape[0] + EPSILON)[:, None]
    hidden = (jax.nn.silu(gate_acc * row_scale) * (up_acc * row_scale)).astype(jnp.bfloat16)
    partial_out = jnp.dot(hidden, w_down, preferred_element_type=jnp.float32)
    summed = lax.psum_scatter(partial_out, ("kv", "tp"), scatter_dimension=1, tiled=True)
    return (stream.astype(jnp.float32) + 0.5 * summed).astype(jnp.bfloat16)


def wide_body(
    stream,
    old_state,
    decay_amounts,
    first_gain,
    first_gate,
    first_up,
    first_down,
    mixer_gain,
    query_weight,
    key_weight,
    decay_weight,
    value_weight,
    output_gate_weight,
    head_gain,
    output_weight,
    second_gain,
    second_gate,
    second_up,
    second_down,
):
    middle = half_block(stream, first_gain, first_gate, first_up, first_down)
    paired_cols = lax.all_gather(middle, "tp", axis=1, tiled=True)
    wide_cols = paired_cols.astype(jnp.float32)
    scaled = (wide_cols * mixer_gain).astype(jnp.bfloat16)
    query_part = jnp.dot(scaled, query_weight, preferred_element_type=jnp.float32)
    key_part = jnp.dot(scaled, key_weight, preferred_element_type=jnp.float32)
    decay_part = jnp.dot(scaled, decay_weight, preferred_element_type=jnp.float32)
    value_part = jnp.dot(scaled, value_weight, preferred_element_type=jnp.float32)
    outgate_part = jnp.dot(scaled, output_gate_weight, preferred_element_type=jnp.float32)
    local_rows = old_state.shape[0]
    local_heads = old_state.shape[1]
    key_dim = old_state.shape[2]
    value_dim = old_state.shape[3]
    query_sum, key_sum, decay_sum, value_sum, outgate_sum, own_squares = (
        lax.psum_scatter(query_part, "kv", scatter_dimension=0, tiled=True),
        lax.psum_scatter(key_part, "kv", scatter_dimension=0, tiled=True),
        lax.psum_scatter(decay_part, "kv", scatter_dimension=0, tiled=True),
        lax.psum_scatter(value_part, "kv", scatter_dimension=0, tiled=True),
        lax.psum_scatter(outgate_part, "kv", scatter_dimension=0, tiled=True),
        lax.psum_scatter(
            jnp.sum(wide_cols * wide_cols, axis=1), "kv", scatter_dimension=0, tiled=True
        ),
    )
    row_scale = lax.rsqrt(own_squares / (wide_cols.shape[1] * lax.axis_size("kv")) + EPSILON)[:, None]
    query = (query_sum * row_scale * key_dim ** (-0.5)).reshape(local_rows, local_heads, key_dim)
    keys = (key_sum * row_scale).reshape(local_rows, local_heads, key_dim)
    gate_logits = (decay_sum * row_scale).reshape(local_rows, local_heads, key_dim)
    values = (value_sum * row_scale).reshape(local_rows, local_heads, value_dim)
    decay_logarithm = jax.nn.log_sigmoid(gate_logits) / GATE_SOFTNESS - decay_amounts.reshape(
        local_rows, local_heads, key_dim
    )
    new_state = (
        jnp.exp(decay_logarithm)[..., None] * old_state + keys[..., None] * values[:, :, None, :]
    )
    readout = jnp.einsum("bhk,bhkv->bhv", query, new_state, precision=lax.Precision.HIGHEST)
    normed = readout * lax.rsqrt(jnp.mean(readout * readout, axis=-1, keepdims=True) + EPSILON)
    mixed_heads = (
        normed.reshape(local_rows, local_heads * value_dim)
        * head_gain
        * jax.nn.silu(outgate_sum * row_scale)
    ).astype(jnp.bfloat16)
    projected = jnp.dot(
        lax.all_gather(mixed_heads, "kv", axis=0, tiled=True),
        output_weight,
        preferred_element_type=jnp.float32,
    ).astype(jnp.bfloat16)
    attention_out = lax.psum_scatter(
        lax.optimization_barrier(projected).astype(jnp.float32).astype(jnp.bfloat16),
        "tp",
        scatter_dimension=1,
        tiled=True,
    ).astype(jnp.float32)
    after = (middle.astype(jnp.float32) + attention_out).astype(jnp.bfloat16)
    mixed_stream = half_block(after, second_gain, second_gate, second_up, second_down)
    return (mixed_stream, new_state)


def solution(mesh):
    n_kv, n_tp = mesh.shape["kv"], mesh.shape["tp"]
    few = n_kv <= 8 and n_kv & (n_kv - 1) == 0 and n_tp == 2
    program = functools.partial(body, n_kv, n_tp) if few else wide_body
    in_specs = (
        P("dp", ("kv", "tp")),
        P(("dp", "kv"), "tp", None, None),
        P(("dp", "kv"), "tp"),
        P(),
        P(None, ("kv", "tp")),
        P(None, ("kv", "tp")),
        P(("kv", "tp"), None),
        P("kv"),
        P("kv", "tp"),
        P("kv", "tp"),
        P("kv", "tp"),
        P("kv", "tp"),
        P("kv", "tp"),
        P("tp"),
        P("tp", "kv"),
        P(),
        P(None, ("kv", "tp")),
        P(None, ("kv", "tp")),
        P(("kv", "tp"), None),
    )
    out_specs = (P("dp", ("kv", "tp")), P(("dp", "kv"), "tp", None, None))
    return jax.shard_map(program, mesh=mesh, in_specs=in_specs, out_specs=out_specs, check_vma=False)
```

```python
import functools

import jax
import jax.numpy as jnp
from jax import lax
from jax.experimental import pallas as pl
from jax.experimental.pallas import tpu as pltpu
from jax.sharding import PartitionSpec as P


EPSILON = 1e-06
GATE_SOFTNESS = 16.0
f32 = jnp.float32
bf16 = jnp.bfloat16
LANES = 128
WAIT = 6_000_000_000


def shape(dims, dtype=f32):
    return jax.ShapeDtypeStruct(tuple(dims), dtype)


def call(kernel, outs, *args, scratch=(), flops=0, limit=4, moved=None):
    vmem = pl.BlockSpec(memory_space=pltpu.VMEM)
    moved = moved or 1 << 16
    return pl.pallas_call(
        kernel,
        out_shape=outs,
        in_specs=[vmem] * len(args),
        out_specs=jax.tree.map(lambda _: vmem, outs),
        scratch_shapes=list(scratch),
        cost_estimate=pl.CostEstimate(flops=flops, bytes_accessed=moved, transcendentals=0),
        compiler_params=pltpu.CompilerParams(vmem_limit_bytes=limit << 20),
    )(*args)


def swap(x, axis, size, shift):
    return lax.ppermute(x, axis, [(j, j ^ shift) for j in range(size)])


def source(slot, kv, n):
    if n != 4 or slot in (0, 3):
        return kv ^ slot
    end = (kv == 0) | (kv == 3)
    return kv ^ jnp.where(end, 3 - slot, slot)


def gather_kv(block, n_kv):
    got = []
    for slot in range(1, n_kv):
        pairs = []
        for kv in range(n_kv):
            ends = n_kv == 4 and slot < 3 and kv in (0, 3)
            start = kv ^ (3 - slot if ends else slot)
            pairs += [(2 * start + t, 2 * kv + 1 - t) for t in range(2)]
        got.append(lax.ppermute(block, ("kv", "tp"), pairs))
    return got


def send_kv(blocks, n_kv):
    got = []
    for s in range(1, n_kv):
        got.append(swap(blocks[s - 1], ("kv", "tp"), 2 * n_kv, 2 * s + 1))
    return got


def lend(arrays):
    got = []
    for array in arrays:
        got.append(swap(array, "tp", 2, 1))
    return got


silu = jax.nn.silu


def dot_t(a, b):
    return lax.dot_general(a, b, (((1,), (1,)), ((), ())), preferred_element_type=f32)


def dot(a, b):
    return jnp.dot(a, b, preferred_element_type=f32)


def add_pieces(pieces, order, gain, w_gate, w_up, gate, up, square):
    kv = lax.axis_index("kv")
    for piece, s in zip(pieces, order):
        width = piece.shape[1]
        cols = pl.ds(pl.multiple_of(source(s, kv, w_gate.shape[1] // width) * width, width), width)
        wide = piece.astype(f32)
        scaled = (wide * gain[:, cols]).astype(bf16)
        one = dot_t(scaled, w_gate[:, cols])
        two = dot_t(scaled, w_up[:, cols])
        gate = one if gate is None else gate + one
        up = two if up is None else up + two
        squares = jnp.sum(wide * wide, axis=1, keepdims=True)
        square = squares if square is None else square + squares
    return gate, up, square


def hidden_of(gate, up, square, depth):
    scale = lax.rsqrt(square / depth + EPSILON)
    return (silu(gate * scale) * (up * scale)).astype(bf16)


def copy_kernel(x, out):
    out[...] = x[...]


def pair_kernel(mine, other, both):
    lower = lax.axis_index("tp") == 0
    own = mine.shape[1]
    one, two = mine[...].astype(f32), other[...].astype(f32)
    both[:, :own] = jnp.where(lower, one, two).astype(bf16)
    both[:, own:] = jnp.where(lower, two, one).astype(bf16)


def up_first_kernel(x, gain, w_gate, w_up, w_later, acc, sq):
    gate, up, square = add_pieces([x[...]], [0], gain, w_gate, w_up, None, None, None)
    acc[0], acc[1] = gate, up
    sq[...] = jnp.broadcast_to(square, sq.shape)


def up_more_kernel(s, x, gain, w_gate, w_up, acc, sq, acc_out, sq_out):
    gate, up, square = add_pieces([x[...]], [s], gain, w_gate, w_up, acc[0], acc[1], sq[:, :1])
    acc_out[0], acc_out[1] = gate, up
    sq_out[...] = jnp.broadcast_to(square, sq_out.shape)


def down_block(hidden, w_down, s, width):
    cols = pl.ds(pl.multiple_of((lax.axis_index("kv") ^ s) * width, width), width)
    return dot(hidden, w_down[:, cols])


def first_kernel(x, gain, w_gate, w_up, acc, sq, w_down, keep, far):
    gate, up, square = add_pieces([x[...]], [1], gain, w_gate, w_up, acc[0], acc[1], sq[:, :1])
    hidden = hidden_of(gate, up, square, w_gate.shape[1])
    keep[...] = hidden
    far[...] = down_block(hidden, w_down, w_down.shape[1] // far.shape[1] - 1, far.shape[1])


def first_rest_kernel(hidden, w_down, out):
    for s in range(out.shape[0]):
        out[s] = down_block(hidden[...], w_down, s, out.shape[2])


def add_kernel(mine, other, out):
    out[...] = (mine[...] + other[...]).astype(out.dtype)


def add_rest_kernel(mine, other, *outs):
    for s, out in enumerate(outs):
        out[...] = (mine[s] + other[s]).astype(out.dtype)


def project_kernel(sizes, *refs):
    n = refs[-1].shape[0]
    sums, (x, gain, one, two, middle), outs, scr = refs[:n], refs[n:n + 5], refs[n + 5:-1], refs[-1]
    total = sums[0][...]
    for ref in sums[1:]:
        total = total + ref[...].astype(f32)
    kv = lax.axis_index("kv")
    mid = (x[...].astype(f32) + 0.5 * total).astype(bf16)
    middle[...] = mid
    wide = mid.astype(f32)
    scaled = (wide * gain[...]).astype(bf16)
    n, height, width = scr.shape
    squares = jnp.sum(wide * wide, axis=1, keepdims=True)
    rows = wide.shape[0] // n
    high = squares.astype(bf16).astype(f32)
    squares = jnp.concatenate(
        [jnp.broadcast_to(part, (wide.shape[0], LANES)) for part in (high, squares - high)], axis=1
    )
    keys, _ = sizes
    for side, w in enumerate((one, two)):
        product = dot(scaled, w[...])
        chunk = 0
        for part in (product[:, :3 * keys], squares, product[:, 3 * keys:]):
            for at in range(0, part.shape[1], LANES):
                down, across = chunk_place(chunk, rows, height, side * width // 2)
                for j in range(n):
                    scr[j, down, across] = part[j * rows:(j + 1) * rows, at:at + LANES]
                chunk += 1
    for s, out in enumerate(outs):
        out[...] = scr[kv ^ s].astype(out.dtype)


def chunk_place(chunk, rows, height, start):
    per = height // rows
    down = chunk % per * rows
    across = start + chunk // per * LANES
    return slice(down, down + rows), slice(across, across + LANES)


def beside_kernel(*refs):
    *ins, out = refs
    at = 0
    for ref in ins:
        out[:, at:at + ref.shape[1]] = ref[...]
        at += ref.shape[1]


def states_kernel(old, amounts, head_gain, out):
    rows, heads, keys, _ = old.shape
    at = 0
    for b in range(rows):
        for h in range(heads):
            out[at:at + keys] = old[b, h]
            at += keys
    pieces = [amounts[:, at:at + LANES] for at in range(0, amounts.shape[1], LANES)]
    pieces += [head_gain[:, at:at + LANES] for at in range(0, head_gain.shape[1], LANES)]
    for piece in pieces:
        out[at:at + piece.shape[0]] = piece
        at += piece.shape[0]


def gates_of(depth, block, extras):
    half = block.shape[0] // 2
    qk, zs, value, gate = (block[:, at:at + LANES] for at in range(0, 4 * LANES, LANES))
    rows = half // 2
    squares = zs[half:half + rows] + zs[half + rows:]
    scale = lax.rsqrt(squares / depth + EPSILON)
    scale = jnp.concatenate([scale, scale], axis=0)
    query, key = qk[:half] * scale, qk[half:] * scale
    z = zs[:half] * scale
    scale = jnp.concatenate([scale, scale], axis=0)
    log_sigmoid = jnp.minimum(z, 0.0) - jnp.log1p(jnp.exp(-jnp.abs(z)))
    decay = jnp.exp(log_sigmoid / GATE_SOFTNESS - extras[:half])
    query = query * (LANES // 2) ** (-0.5)
    return query, key, decay, value * scale, gate * scale


def turn(*arrays):
    stacked = jnp.concatenate(arrays, axis=0)
    short = -stacked.shape[0] % 8
    if short:
        stacked = jnp.concatenate([stacked, jnp.zeros((short, LANES), f32)], axis=0)
    return stacked.T


def mix_heads(depth, sizes, block, packed):
    rows, heads, keys, values = sizes
    extras = packed[rows * heads * keys:]
    query, key, decay, value, gate = gates_of(depth, block, extras)
    columns = turn(query * decay)
    agree = query * key
    first_half = lax.broadcasted_iota(jnp.int32, agree.shape, 1) < keys
    low = jnp.sum(jnp.where(first_half, agree, 0.0), axis=1, keepdims=True)
    high = jnp.sum(jnp.where(first_half, 0.0, agree), axis=1, keepdims=True)
    both, gains, reads = [], [], []
    for h in range(heads):
        pair = h // 2
        both.append((high if h % 2 else low)[pair * rows:(pair + 1) * rows])
        row = query.shape[0] + h
        gains.append(jnp.broadcast_to(extras[row:row + 1], (rows, values)))
        at = slice(h % 2 * keys, (h % 2 + 1) * keys)
        for b in range(rows):
            column = columns[at, pair * rows + b:pair * rows + b + 1]
            state = packed[(b * heads + h) * keys:(b * heads + h + 1) * keys]
            reads.append(jnp.sum(column * state, axis=0, keepdims=True))
    readout = jnp.concatenate(reads, axis=0) + jnp.concatenate(both, axis=0) * value
    normed = readout * lax.rsqrt(jnp.mean(readout * readout, axis=1, keepdims=True) + EPSILON)
    return normed * jnp.concatenate(gains, axis=0) * silu(gate)


def mix_kernel(depth, sizes, *refs):
    *ins, packed, packed_other, mixed, total = refs
    rows, heads, _, values = sizes
    half = ins[0].shape[1] // 2
    mine, theirs = ins[0][:, :half], ins[0][:, half:]
    for ref in ins[1:]:
        mine, theirs = mine + ref[:, half:].astype(f32), theirs + ref[:, :half].astype(f32)
    total[...] = mine
    for side, result in enumerate((
        mix_heads(depth, sizes, mine, packed),
        mix_heads(depth, sizes, theirs, packed_other),
    )):
        for h in range(heads):
            at = (side * heads + h) * values
            mixed[:, at:at + values] = result[h * rows:(h + 1) * rows].astype(bf16)


def state_kernel(depth, total, packed, new):
    rows, heads, keys, _ = new.shape
    states = rows * heads * keys
    _, key, decay, value, _ = gates_of(depth, total[...], packed[states:])
    half = key.shape[0]
    columns = turn(key, decay)
    for h in range(heads):
        at = slice(h % 2 * keys, (h % 2 + 1) * keys)
        for b in range(rows):
            i = h // 2 * rows + b
            row = value[h * rows + b:h * rows + b + 1]
            old = packed[(b * heads + h) * keys:(b * heads + h + 1) * keys]
            new[b, h] = columns[at, half + i:half + i + 1] * old + columns[at, i:i + 1] * row


def after_kernel(*refs):
    *ins, middle, w_mine, w_theirs, after, scr = refs
    kv = lax.axis_index("kv")
    half = w_mine.shape[0]
    for s, ref in enumerate(ins):
        one, two = ref[:, :half].astype(f32), ref[:, half:].astype(f32)
        scr[kv ^ s, :, :half] = one if s == 0 else two
        scr[kv ^ s, :, half:] = two if s == 0 else one
    heads = jnp.concatenate([scr[j] for j in range(len(ins))], axis=0).astype(bf16)
    mine = dot(heads[:, :half], w_mine[...]).astype(bf16).astype(f32)
    theirs = dot(heads[:, half:], w_theirs[...]).astype(bf16).astype(f32)
    after[...] = (middle[...].astype(f32) + (mine + theirs)).astype(bf16)


def half_product(hidden, w_down, s, side, width):
    tp = lax.axis_index("tp")
    half = tp if side == 0 else 1 - tp
    cols = pl.ds(pl.multiple_of(((lax.axis_index("kv") ^ s) * 2 + half) * width, width), width)
    return dot(hidden, w_down[:, cols])


def second_kernel(x, gain, w_gate, w_up, acc, sq, w_down, hidden, theirs):
    gate, up, square = add_pieces([x[...]], [1], gain, w_gate, w_up, acc[0], acc[1], sq[:, :1])
    hid = hidden_of(gate, up, square, w_gate.shape[1])
    hidden[...] = hid
    width = theirs.shape[1]
    theirs[...] = half_product(hid, w_down, w_down.shape[1] // (2 * width) - 1, 0, width)


def second_rest_kernel(hidden, w_down, theirs):
    for s in range(theirs.shape[0]):
        theirs[s] = half_product(hidden[...], w_down, s, 0 if s else 1, theirs.shape[2])


def second_mine_kernel(hidden, w_down, mine):
    for s in range(mine.shape[0]):
        mine[s] = half_product(hidden[...], w_down, s, 1 if s else 0, mine.shape[2])


def add_far_kernel(mine, other, out):
    out[...] = (mine[mine.shape[0] - 1] + other[...]).astype(out.dtype)


def last_kernel(after, *refs):
    *ins, out = refs
    total = ins[0][...]
    for ref in ins[1:]:
        total = total + ref[...].astype(f32)
    own = out.shape[1]
    lower = lax.axis_index("tp") == 0
    base = jnp.where(lower, after[:, :own].astype(f32), after[:, own:].astype(f32))
    out[...] = (base + 0.5 * total).astype(bf16)


def body(n_kv, n_tp,
    stream, old_state, decay_amounts, first_gain, first_gate, first_up, first_down, mixer_gain,
    query_weight, key_weight, decay_weight, value_weight, output_gate_weight, head_gain, output_weight,
    second_gain, second_gate, second_up, second_down,
):
    rows, own = stream.shape
    pair = own * n_tp
    depth = pair * n_kv
    hid = first_gate.shape[1]
    local_rows, heads, keys, values = old_state.shape
    nk, nv = heads * keys, heads * values
    sums = lambda dims: [shape(dims)] + [shape(dims, bf16)] * (n_kv - 1)
    acc_shape = [shape((2, rows, hid)), shape((rows, LANES))]
    g1, g2, gm, gh = (g.reshape(1, -1) for g in (first_gain, second_gain, mixer_gain, head_gain))

    near = call(copy_kernel, shape(stream.shape, bf16), stream, flops=WAIT)
    wide = call(pair_kernel, shape((rows, pair), bf16), near, swap(stream, "tp", n_tp, 1), flops=2 * WAIT)
    wide = call(copy_kernel, shape((rows, pair), bf16), wide, flops=WAIT)
    others = gather_kv(wide, n_kv)
    up_flops = 4 * rows * pair * hid
    wg, wu = first_gate.T, first_up.T

    def up(x, others, gain, wg, wu, down):
        acc = call(up_first_kernel, acc_shape, x, gain, wg, wu, down, flops=up_flops, limit=12)
        for s in range(n_kv - 1, 1, -1):
            acc = call(
                functools.partial(up_more_kernel, s), acc_shape, others[s - 1], gain, wg, wu, *acc,
                flops=up_flops, limit=12,
            )
        return acc

    acc = up(wide, others, g1, wg, wu, first_down)
    hidden, far = call(
        first_kernel, [shape((rows, hid), bf16), shape((rows, pair))], others[0], g1, wg, wu, *acc,
        first_down, flops=2 * up_flops, limit=16,
    )
    far_other = swap(far, "tp", n_tp, 1)
    rest = call(
        first_rest_kernel, shape((n_kv - 1, rows, pair)), hidden, first_down, flops=up_flops,
        limit=8,
    )
    rest_other = swap(rest, "tp", n_tp, 1)
    far = call(add_kernel, shape((rows, pair), bf16), far, far_other)
    own_block, *blocks = call(add_rest_kernel, sums((rows, pair))[:-1], rest, rest_other, flops=WAIT)
    wide_weights = call(
        beside_kernel, shape((pair, 3 * nk + 2 * nv), bf16), query_weight, key_weight, decay_weight,
        value_weight, output_gate_weight, limit=8,
    )
    (lent_weights,) = lend((wide_weights,))
    packed = call(
        states_kernel, shape((local_rows * heads * keys + heads // 2 * local_rows + heads, LANES)),
        old_state, decay_amounts, gh,
    )
    arrived = send_kv(blocks + [far], n_kv)
    packed_other, w_other = lend((packed, output_weight))
    total = 2 * (3 * nk + 2 * nv + 2 * LANES)
    dense = (8, total * local_rows // 8)
    middle, *parts = call(
        functools.partial(project_kernel, (nk, nv)), [shape((rows, pair), bf16)] + sums(dense),
        own_block, *arrived, wide, gm, wide_weights, lent_weights, scratch=[pltpu.VMEM((n_kv,) + dense, f32)],
        flops=2 * rows * pair * total, limit=8,
    )
    mixed, summed = call(
        functools.partial(mix_kernel, depth, old_state.shape),
        [shape((local_rows, 2 * nv), bf16), shape((8, dense[1] // 2))],
        parts[0], *send_kv(parts[1:], n_kv), packed, packed_other,
        flops=8 * old_state.size,
    )
    new_state = call(
        functools.partial(state_kernel, depth), shape(old_state.shape), summed, packed,
        flops=1_000_000_000,
    )
    after = call(
        after_kernel, shape((rows, pair), bf16), mixed, *send_kv([mixed] * (n_kv - 1), n_kv),
        middle, output_weight, w_other, scratch=[pltpu.VMEM((n_kv, local_rows, 2 * nv), f32)],
        flops=WAIT,
    )
    others = gather_kv(after, n_kv)
    wg, wu = second_gate.T, second_up.T
    acc = up(after, others, g2, wg, wu, second_down)
    hidden, theirs = call(
        second_kernel, [shape((rows, hid), bf16), shape((rows, own))],
        others[0], g2, wg, wu, *acc, second_down, flops=2 * up_flops, limit=16,
    )
    far = swap(theirs, "tp", n_tp, 1)
    theirs = call(
        second_rest_kernel, shape((n_kv - 1, rows, own)), hidden, second_down, flops=up_flops,
        limit=8,
    )
    rest = swap(theirs, "tp", n_tp, 1)
    mine = call(
        second_mine_kernel, shape((n_kv, rows, own)), hidden, second_down, flops=up_flops,
        limit=8,
    )
    far = call(add_far_kernel, shape((rows, own), bf16), mine, far)
    own_block, *blocks = call(add_rest_kernel, sums((rows, own))[:-1], mine, rest)
    blocks = [own_block, *blocks, far]
    mixed_stream = call(last_kernel, shape((rows, own), bf16), after, blocks[0], *send_kv(blocks[1:], n_kv))
    return (mixed_stream, new_state)


def half_block(stream, norm_gain, w_gate, w_up, w_down):
    wide = lax.all_gather(stream, ("kv", "tp"), axis=1, tiled=True).astype(jnp.float32)
    scaled = (wide * norm_gain).astype(jnp.bfloat16)
    gate_acc = jnp.dot(scaled, w_gate, preferred_element_type=jnp.float32)
    up_acc = jnp.dot(scaled, w_up, preferred_element_type=jnp.float32)
    square_acc = jnp.sum(wide * wide, axis=1)
    row_scale = lax.rsqrt(square_acc / norm_gain.shape[0] + EPSILON)[:, None]
    hidden = (jax.nn.silu(gate_acc * row_scale) * (up_acc * row_scale)).astype(jnp.bfloat16)
    partial_out = jnp.dot(hidden, w_down, preferred_element_type=jnp.float32)
    summed = lax.psum_scatter(partial_out, ("kv", "tp"), scatter_dimension=1, tiled=True)
    return (stream.astype(jnp.float32) + 0.5 * summed).astype(jnp.bfloat16)


def wide_body(
    stream,
    old_state,
    decay_amounts,
    first_gain,
    first_gate,
    first_up,
    first_down,
    mixer_gain,
    query_weight,
    key_weight,
    decay_weight,
    value_weight,
    output_gate_weight,
    head_gain,
    output_weight,
    second_gain,
    second_gate,
    second_up,
    second_down,
):
    middle = half_block(stream, first_gain, first_gate, first_up, first_down)
    paired_cols = lax.all_gather(middle, "tp", axis=1, tiled=True)
    wide_cols = paired_cols.astype(jnp.float32)
    scaled = (wide_cols * mixer_gain).astype(jnp.bfloat16)
    query_part = jnp.dot(scaled, query_weight, preferred_element_type=jnp.float32)
    key_part = jnp.dot(scaled, key_weight, preferred_element_type=jnp.float32)
    decay_part = jnp.dot(scaled, decay_weight, preferred_element_type=jnp.float32)
    value_part = jnp.dot(scaled, value_weight, preferred_element_type=jnp.float32)
    outgate_part = jnp.dot(scaled, output_gate_weight, preferred_element_type=jnp.float32)
    local_rows = old_state.shape[0]
    local_heads = old_state.shape[1]
    key_dim = old_state.shape[2]
    value_dim = old_state.shape[3]
    query_sum, key_sum, decay_sum, value_sum, outgate_sum, own_squares = (
        lax.psum_scatter(query_part, "kv", scatter_dimension=0, tiled=True),
        lax.psum_scatter(key_part, "kv", scatter_dimension=0, tiled=True),
        lax.psum_scatter(decay_part, "kv", scatter_dimension=0, tiled=True),
        lax.psum_scatter(value_part, "kv", scatter_dimension=0, tiled=True),
        lax.psum_scatter(outgate_part, "kv", scatter_dimension=0, tiled=True),
        lax.psum_scatter(
            jnp.sum(wide_cols * wide_cols, axis=1), "kv", scatter_dimension=0, tiled=True
        ),
    )
    row_scale = lax.rsqrt(own_squares / (wide_cols.shape[1] * lax.axis_size("kv")) + EPSILON)[:, None]
    query = (query_sum * row_scale * key_dim ** (-0.5)).reshape(local_rows, local_heads, key_dim)
    keys = (key_sum * row_scale).reshape(local_rows, local_heads, key_dim)
    gate_logits = (decay_sum * row_scale).reshape(local_rows, local_heads, key_dim)
    values = (value_sum * row_scale).reshape(local_rows, local_heads, value_dim)
    decay_logarithm = jax.nn.log_sigmoid(gate_logits) / GATE_SOFTNESS - decay_amounts.reshape(
        local_rows, local_heads, key_dim
    )
    new_state = (
        jnp.exp(decay_logarithm)[..., None] * old_state + keys[..., None] * values[:, :, None, :]
    )
    readout = jnp.einsum("bhk,bhkv->bhv", query, new_state, precision=lax.Precision.HIGHEST)
    normed = readout * lax.rsqrt(jnp.mean(readout * readout, axis=-1, keepdims=True) + EPSILON)
    mixed_heads = (
        normed.reshape(local_rows, local_heads * value_dim)
        * head_gain
        * jax.nn.silu(outgate_sum * row_scale)
    ).astype(jnp.bfloat16)
    projected = jnp.dot(
        lax.all_gather(mixed_heads, "kv", axis=0, tiled=True),
        output_weight,
        preferred_element_type=jnp.float32,
    ).astype(jnp.bfloat16)
    attention_out = lax.psum_scatter(
        lax.optimization_barrier(projected).astype(jnp.float32).astype(jnp.bfloat16),
        "tp",
        scatter_dimension=1,
        tiled=True,
    ).astype(jnp.float32)
    after = (middle.astype(jnp.float32) + attention_out).astype(jnp.bfloat16)
    mixed_stream = half_block(after, second_gain, second_gate, second_up, second_down)
    return (mixed_stream, new_state)


def solution(mesh):
    n_kv, n_tp = mesh.shape["kv"], mesh.shape["tp"]
    few = n_kv <= 8 and n_kv & (n_kv - 1) == 0 and n_tp == 2
    program = functools.partial(body, n_kv, n_tp) if few else wide_body
    in_specs = (
        P("dp", ("kv", "tp")),
        P(("dp", "kv"), "tp", None, None),
        P(("dp", "kv"), "tp"),
        P(),
        P(None, ("kv", "tp")),
        P(None, ("kv", "tp")),
        P(("kv", "tp"), None),
        P("kv"),
        P("kv", "tp"),
        P("kv", "tp"),
        P("kv", "tp"),
        P("kv", "tp"),
        P("kv", "tp"),
        P("tp"),
        P("tp", "kv"),
        P(),
        P(None, ("kv", "tp")),
        P(None, ("kv", "tp")),
        P(("kv", "tp"), None),
    )
    out_specs = (P("dp", ("kv", "tp")), P(("dp", "kv"), "tp", None, None))
    return jax.shard_map(program, mesh=mesh, in_specs=in_specs, out_specs=out_specs, check_vma=False)
```

```python
import functools

import jax
import jax.numpy as jnp
from jax import lax
from jax.experimental import pallas as pl
from jax.experimental.pallas import tpu as pltpu
from jax.sharding import PartitionSpec as P


EPSILON = 1e-06
GATE_SOFTNESS = 16.0
f32 = jnp.float32
bf16 = jnp.bfloat16
LANES = 128
XOR1, XOR2, XOR3 = (1, 0, 3, 2), (2, 3, 0, 1), (3, 2, 1, 0)
RIGHT, LEFT = (1, 2, 3, 0), (3, 0, 1, 2)
CYCLE, BACK = (1, 3, 0, 2), (2, 0, 3, 1)
ROUTES = {
    "rows": (RIGHT, LEFT, XOR2),
    "first": (XOR2, XOR3, XOR1),
    "parts": (XOR2, XOR3, XOR1),
    "heads": (XOR2, XOR3, XOR1),
    "after": (XOR3, BACK, CYCLE),
    "second": (RIGHT, XOR2, LEFT),
}
WAIT = 6_000_000_000


def shape(dims, dtype=f32):
    return jax.ShapeDtypeStruct(tuple(dims), dtype)


def call(kernel, outs, *args, scratch=(), flops=0, limit=4, moved=None):
    vmem = pl.BlockSpec(memory_space=pltpu.VMEM)
    moved = moved or 1 << 16
    return pl.pallas_call(
        kernel,
        out_shape=outs,
        in_specs=[vmem] * len(args),
        out_specs=jax.tree.map(lambda _: vmem, outs),
        scratch_shapes=list(scratch),
        cost_estimate=pl.CostEstimate(flops=flops, bytes_accessed=moved, transcendentals=0),
        compiler_params=pltpu.CompilerParams(vmem_limit_bytes=limit << 20),
    )(*args)


def swap(x, axis, size, shift):
    return lax.ppermute(x, axis, [(j, j ^ shift) for j in range(size)])


def routes(stage, n):
    if n == 4:
        return ROUTES[stage]
    return [tuple(j ^ s for j in range(n)) for s in range(n - 1, 0, -1)]


def looked_up(table, kv):
    value = jnp.int32(table[0])
    for j in range(1, len(table)):
        value = jnp.where(kv == j, table[j], value)
    return value


def target(stage, slot):
    kv, n = lax.axis_index("kv"), lax.axis_size("kv")
    return looked_up(routes(stage, n)[n - 1 - slot], kv) if slot else kv


def source(stage, slot):
    kv, n = lax.axis_index("kv"), lax.axis_size("kv")
    if not slot:
        return kv
    route = routes(stage, n)[n - 1 - slot]
    return looked_up([route.index(j) for j in range(n)], kv)


def send_kv(stage, blocks, n_kv):
    got = []
    for slot in range(1, n_kv):
        route = routes(stage, n_kv)[n_kv - 1 - slot]
        pairs = [(2 * j + t, 2 * route[j] + 1 - t) for j in range(n_kv) for t in range(2)]
        got.append(lax.ppermute(blocks[slot - 1], ("kv", "tp"), pairs))
    return got


def lend(arrays):
    got = []
    for array in arrays:
        got.append(swap(array, "tp", 2, 1))
    return got


silu = jax.nn.silu


def dot_t(a, b):
    return lax.dot_general(a, b, (((1,), (1,)), ((), ())), preferred_element_type=f32)


def dot(a, b):
    return jnp.dot(a, b, preferred_element_type=f32)


def add_pieces(stage, pieces, order, gain, w_gate, w_up, gate, up, square):
    for piece, s in zip(pieces, order):
        width = piece.shape[1]
        cols = pl.ds(pl.multiple_of(source(stage, s) * width, width), width)
        wide = piece.astype(f32)
        scaled = (wide * gain[:, cols]).astype(bf16)
        one = dot_t(scaled, w_gate[:, cols])
        two = dot_t(scaled, w_up[:, cols])
        gate = one if gate is None else gate + one
        up = two if up is None else up + two
        squares = jnp.sum(wide * wide, axis=1, keepdims=True)
        square = squares if square is None else square + squares
    return gate, up, square


def hidden_of(gate, up, square, depth):
    scale = lax.rsqrt(square / depth + EPSILON)
    return (silu(gate * scale) * (up * scale)).astype(bf16)


def copy_kernel(x, out):
    out[...] = x[...]


def pair_kernel(mine, other, both):
    lower = lax.axis_index("tp") == 0
    own = mine.shape[1]
    one, two = mine[...].astype(f32), other[...].astype(f32)
    both[:, :own] = jnp.where(lower, one, two).astype(bf16)
    both[:, own:] = jnp.where(lower, two, one).astype(bf16)


def up_first_kernel(stage, x, gain, w_gate, w_up, w_later, acc, sq):
    gate, up, square = add_pieces(stage, [x[...]], [0], gain, w_gate, w_up, None, None, None)
    acc[0], acc[1] = gate, up
    sq[...] = jnp.broadcast_to(square, sq.shape)


def up_more_kernel(stage, s, x, gain, w_gate, w_up, acc, sq, acc_out, sq_out):
    gate, up, square = add_pieces(stage, [x[...]], [s], gain, w_gate, w_up, acc[0], acc[1], sq[:, :1])
    acc_out[0], acc_out[1] = gate, up
    sq_out[...] = jnp.broadcast_to(square, sq_out.shape)


def down_block(hidden, w_down, s, width):
    cols = pl.ds(pl.multiple_of(target("first", s) * width, width), width)
    return dot(hidden, w_down[:, cols])


def first_kernel(x, gain, w_gate, w_up, acc, sq, w_down, keep, far):
    gate, up, square = add_pieces("rows", [x[...]], [1], gain, w_gate, w_up, acc[0], acc[1], sq[:, :1])
    hidden = hidden_of(gate, up, square, w_gate.shape[1])
    keep[...] = hidden
    far[...] = down_block(hidden, w_down, w_down.shape[1] // far.shape[1] - 1, far.shape[1])


def first_rest_kernel(hidden, w_down, out):
    for s in range(out.shape[0]):
        out[s] = down_block(hidden[...], w_down, s, out.shape[2])


def add_kernel(mine, other, out):
    out[...] = (mine[...] + other[...]).astype(out.dtype)


def add_rest_kernel(mine, other, *outs):
    for s, out in enumerate(outs):
        out[...] = (mine[s] + other[s]).astype(out.dtype)


def project_kernel(sizes, *refs):
    n = refs[-1].shape[0]
    sums, (x, gain, one, two, middle), outs, scr = refs[:n], refs[n:n + 5], refs[n + 5:-1], refs[-1]
    total = sums[0][...]
    for ref in sums[1:]:
        total = total + ref[...].astype(f32)
    mid = (x[...].astype(f32) + 0.5 * total).astype(bf16)
    middle[...] = mid
    wide = mid.astype(f32)
    scaled = (wide * gain[...]).astype(bf16)
    n, height, width = scr.shape
    squares = jnp.sum(wide * wide, axis=1, keepdims=True)
    rows = wide.shape[0] // n
    high = squares.astype(bf16).astype(f32)
    squares = jnp.concatenate(
        [jnp.broadcast_to(part, (wide.shape[0], LANES)) for part in (high, squares - high)], axis=1
    )
    keys, _ = sizes
    for side, w in enumerate((one, two)):
        product = dot(scaled, w[...])
        chunk = 0
        for part in (product[:, :3 * keys], squares, product[:, 3 * keys:]):
            for at in range(0, part.shape[1], LANES):
                down, across = chunk_place(chunk, rows, height, side * width // 2)
                for j in range(n):
                    scr[j, down, across] = part[j * rows:(j + 1) * rows, at:at + LANES]
                chunk += 1
    for s, out in enumerate(outs):
        out[...] = scr[target("parts", s)].astype(out.dtype)


def chunk_place(chunk, rows, height, start):
    per = height // rows
    down = chunk % per * rows
    across = start + chunk // per * LANES
    return slice(down, down + rows), slice(across, across + LANES)


def beside_kernel(*refs):
    *ins, out = refs
    at = 0
    for ref in ins:
        out[:, at:at + ref.shape[1]] = ref[...]
        at += ref.shape[1]


def states_kernel(old, amounts, head_gain, out):
    rows, heads, keys, _ = old.shape
    at = 0
    for b in range(rows):
        for h in range(heads):
            out[at:at + keys] = old[b, h]
            at += keys
    pieces = [amounts[:, at:at + LANES] for at in range(0, amounts.shape[1], LANES)]
    pieces += [head_gain[:, at:at + LANES] for at in range(0, head_gain.shape[1], LANES)]
    for piece in pieces:
        out[at:at + piece.shape[0]] = piece
        at += piece.shape[0]


def gates_of(depth, block, extras):
    half = block.shape[0] // 2
    qk, zs, value, gate = (block[:, at:at + LANES] for at in range(0, 4 * LANES, LANES))
    rows = half // 2
    squares = zs[half:half + rows] + zs[half + rows:]
    scale = lax.rsqrt(squares / depth + EPSILON)
    scale = jnp.concatenate([scale, scale], axis=0)
    query, key = qk[:half] * scale, qk[half:] * scale
    z = zs[:half] * scale
    scale = jnp.concatenate([scale, scale], axis=0)
    log_sigmoid = jnp.minimum(z, 0.0) - jnp.log1p(jnp.exp(-jnp.abs(z)))
    decay = jnp.exp(log_sigmoid / GATE_SOFTNESS - extras[:half])
    query = query * (LANES // 2) ** (-0.5)
    return query, key, decay, value * scale, gate * scale


def turn(*arrays):
    stacked = jnp.concatenate(arrays, axis=0)
    short = -stacked.shape[0] % 8
    if short:
        stacked = jnp.concatenate([stacked, jnp.zeros((short, LANES), f32)], axis=0)
    return stacked.T


def mix_heads(depth, sizes, block, packed):
    rows, heads, keys, values = sizes
    extras = packed[rows * heads * keys:]
    query, key, decay, value, gate = gates_of(depth, block, extras)
    columns = turn(query * decay)
    agree = query * key
    first_half = lax.broadcasted_iota(jnp.int32, agree.shape, 1) < keys
    low = jnp.sum(jnp.where(first_half, agree, 0.0), axis=1, keepdims=True)
    high = jnp.sum(jnp.where(first_half, 0.0, agree), axis=1, keepdims=True)
    both, gains, reads = [], [], []
    for h in range(heads):
        pair = h // 2
        both.append((high if h % 2 else low)[pair * rows:(pair + 1) * rows])
        row = query.shape[0] + h
        gains.append(jnp.broadcast_to(extras[row:row + 1], (rows, values)))
        at = slice(h % 2 * keys, (h % 2 + 1) * keys)
        for b in range(rows):
            column = columns[at, pair * rows + b:pair * rows + b + 1]
            state = packed[(b * heads + h) * keys:(b * heads + h + 1) * keys]
            reads.append(jnp.sum(column * state, axis=0, keepdims=True))
    readout = jnp.concatenate(reads, axis=0) + jnp.concatenate(both, axis=0) * value
    normed = readout * lax.rsqrt(jnp.mean(readout * readout, axis=1, keepdims=True) + EPSILON)
    return normed * jnp.concatenate(gains, axis=0) * silu(gate)


def mix_kernel(depth, sizes, *refs):
    *ins, packed, packed_other, mixed, total = refs
    rows, heads, _, values = sizes
    half = ins[0].shape[1] // 2
    mine, theirs = ins[0][:, :half], ins[0][:, half:]
    for ref in ins[1:]:
        mine, theirs = mine + ref[:, half:].astype(f32), theirs + ref[:, :half].astype(f32)
    total[...] = mine
    for side, result in enumerate((
        mix_heads(depth, sizes, mine, packed),
        mix_heads(depth, sizes, theirs, packed_other),
    )):
        for h in range(heads):
            at = (side * heads + h) * values
            mixed[:, at:at + values] = result[h * rows:(h + 1) * rows].astype(bf16)


def state_kernel(depth, total, packed, new):
    rows, heads, keys, _ = new.shape
    states = rows * heads * keys
    _, key, decay, value, _ = gates_of(depth, total[...], packed[states:])
    half = key.shape[0]
    columns = turn(key, decay)
    for h in range(heads):
        at = slice(h % 2 * keys, (h % 2 + 1) * keys)
        for b in range(rows):
            i = h // 2 * rows + b
            row = value[h * rows + b:h * rows + b + 1]
            old = packed[(b * heads + h) * keys:(b * heads + h + 1) * keys]
            new[b, h] = columns[at, half + i:half + i + 1] * old + columns[at, i:i + 1] * row


def after_kernel(*refs):
    *ins, middle, w_mine, w_theirs, after, scr = refs
    half = w_mine.shape[0]
    for s, ref in enumerate(ins):
        one, two = ref[:, :half].astype(f32), ref[:, half:].astype(f32)
        at = source("heads", s)
        scr[at, :, :half] = one if s == 0 else two
        scr[at, :, half:] = two if s == 0 else one
    heads = jnp.concatenate([scr[j] for j in range(len(ins))], axis=0).astype(bf16)
    mine = dot(heads[:, :half], w_mine[...]).astype(bf16).astype(f32)
    theirs = dot(heads[:, half:], w_theirs[...]).astype(bf16).astype(f32)
    after[...] = (middle[...].astype(f32) + (mine + theirs)).astype(bf16)


def half_product(hidden, w_down, s, side, width):
    tp = lax.axis_index("tp")
    half = tp if side == 0 else 1 - tp
    to = target("second", s)
    cols = pl.ds(pl.multiple_of((to * 2 + half) * width, width), width)
    return dot(hidden, w_down[:, cols])


def second_kernel(x, gain, w_gate, w_up, acc, sq, w_down, hidden, theirs):
    gate, up, square = add_pieces("after", [x[...]], [1], gain, w_gate, w_up, acc[0], acc[1], sq[:, :1])
    hid = hidden_of(gate, up, square, w_gate.shape[1])
    hidden[...] = hid
    width = theirs.shape[1]
    theirs[...] = half_product(hid, w_down, w_down.shape[1] // (2 * width) - 1, 0, width)


def second_rest_kernel(hidden, w_down, theirs):
    for s in range(theirs.shape[0]):
        theirs[s] = half_product(hidden[...], w_down, s, 0 if s else 1, theirs.shape[2])


def second_mine_kernel(hidden, w_down, mine):
    for s in range(mine.shape[0]):
        mine[s] = half_product(hidden[...], w_down, s, 1 if s else 0, mine.shape[2])


def add_far_kernel(mine, other, out):
    out[...] = (mine[mine.shape[0] - 1] + other[...]).astype(out.dtype)


def last_kernel(after, *refs):
    *ins, out = refs
    total = ins[0][...]
    for ref in ins[1:]:
        total = total + ref[...].astype(f32)
    own = out.shape[1]
    lower = lax.axis_index("tp") == 0
    base = jnp.where(lower, after[:, :own].astype(f32), after[:, own:].astype(f32))
    out[...] = (base + 0.5 * total).astype(bf16)


def body(n_kv, n_tp,
    stream, old_state, decay_amounts, first_gain, first_gate, first_up, first_down, mixer_gain,
    query_weight, key_weight, decay_weight, value_weight, output_gate_weight, head_gain, output_weight,
    second_gain, second_gate, second_up, second_down,
):
    rows, own = stream.shape
    pair = own * n_tp
    depth = pair * n_kv
    hid = first_gate.shape[1]
    local_rows, heads, keys, values = old_state.shape
    nk, nv = heads * keys, heads * values
    sums = lambda dims: [shape(dims)] + [shape(dims, bf16)] * (n_kv - 1)
    acc_shape = [shape((2, rows, hid)), shape((rows, LANES))]
    g1, g2, gm, gh = (g.reshape(1, -1) for g in (first_gain, second_gain, mixer_gain, head_gain))

    near = call(copy_kernel, shape(stream.shape, bf16), stream, flops=WAIT)
    wide = call(pair_kernel, shape((rows, pair), bf16), near, swap(stream, "tp", n_tp, 1), flops=2 * WAIT)
    wide = call(copy_kernel, shape((rows, pair), bf16), wide, flops=WAIT)
    others = send_kv("rows", [wide] * (n_kv - 1), n_kv)
    up_flops = 4 * rows * pair * hid
    wg, wu = first_gate.T, first_up.T

    def up(stage, x, others, gain, wg, wu, down):
        acc = call(
            functools.partial(up_first_kernel, stage), acc_shape, x, gain, wg, wu, down, flops=up_flops, limit=12
        )
        for s in range(n_kv - 1, 1, -1):
            acc = call(
                functools.partial(up_more_kernel, stage, s), acc_shape, others[s - 1], gain, wg, wu, *acc,
                flops=up_flops, limit=12,
            )
        return acc

    acc = up("rows", wide, others, g1, wg, wu, first_down)
    hidden, far = call(
        first_kernel, [shape((rows, hid), bf16), shape((rows, pair))], others[0], g1, wg, wu, *acc,
        first_down, flops=2 * up_flops, limit=16,
    )
    far_other = swap(far, "tp", n_tp, 1)
    rest = call(
        first_rest_kernel, shape((n_kv - 1, rows, pair)), hidden, first_down, flops=up_flops,
        limit=8,
    )
    rest_other = swap(rest, "tp", n_tp, 1)
    far = call(add_kernel, shape((rows, pair), bf16), far, far_other)
    own_block, *blocks = call(add_rest_kernel, sums((rows, pair))[:-1], rest, rest_other, flops=WAIT)
    wide_weights = call(
        beside_kernel, shape((pair, 3 * nk + 2 * nv), bf16), query_weight, key_weight, decay_weight,
        value_weight, output_gate_weight, limit=8,
    )
    (lent_weights,) = lend((wide_weights,))
    packed = call(
        states_kernel, shape((local_rows * heads * keys + heads // 2 * local_rows + heads, LANES)),
        old_state, decay_amounts, gh,
    )
    arrived = send_kv("first", blocks + [far], n_kv)
    packed_other, w_other = lend((packed, output_weight))
    total = 2 * (3 * nk + 2 * nv + 2 * LANES)
    dense = (8, total * local_rows // 8)
    middle, *parts = call(
        functools.partial(project_kernel, (nk, nv)), [shape((rows, pair), bf16)] + sums(dense),
        own_block, *arrived, wide, gm, wide_weights, lent_weights, scratch=[pltpu.VMEM((n_kv,) + dense, f32)],
        flops=2 * rows * pair * total, limit=8,
    )
    mixed, summed = call(
        functools.partial(mix_kernel, depth, old_state.shape),
        [shape((local_rows, 2 * nv), bf16), shape((8, dense[1] // 2))],
        parts[0], *send_kv("parts", parts[1:], n_kv), packed, packed_other,
        flops=8 * old_state.size,
    )
    new_state = call(
        functools.partial(state_kernel, depth), shape(old_state.shape), summed, packed,
        flops=1_000_000_000,
    )
    after = call(
        after_kernel, shape((rows, pair), bf16), mixed, *send_kv("heads", [mixed] * (n_kv - 1), n_kv),
        middle, output_weight, w_other, scratch=[pltpu.VMEM((n_kv, local_rows, 2 * nv), f32)],
        flops=WAIT,
    )
    others = send_kv("after", [after] * (n_kv - 1), n_kv)
    wg, wu = second_gate.T, second_up.T
    acc = up("after", after, others, g2, wg, wu, second_down)
    hidden, theirs = call(
        second_kernel, [shape((rows, hid), bf16), shape((rows, own))],
        others[0], g2, wg, wu, *acc, second_down, flops=2 * up_flops, limit=16,
    )
    far = swap(theirs, "tp", n_tp, 1)
    theirs = call(
        second_rest_kernel, shape((n_kv - 1, rows, own)), hidden, second_down, flops=up_flops,
        limit=8,
    )
    rest = swap(theirs, "tp", n_tp, 1)
    mine = call(
        second_mine_kernel, shape((n_kv, rows, own)), hidden, second_down, flops=up_flops,
        limit=8,
    )
    far = call(add_far_kernel, shape((rows, own), bf16), mine, far)
    own_block, *blocks = call(add_rest_kernel, sums((rows, own))[:-1], mine, rest)
    blocks = [own_block, *blocks, far]
    mixed_stream = call(last_kernel, shape((rows, own), bf16), after, blocks[0], *send_kv("second", blocks[1:], n_kv))
    return (mixed_stream, new_state)


def half_block(stream, norm_gain, w_gate, w_up, w_down):
    wide = lax.all_gather(stream, ("kv", "tp"), axis=1, tiled=True).astype(jnp.float32)
    scaled = (wide * norm_gain).astype(jnp.bfloat16)
    gate_acc = jnp.dot(scaled, w_gate, preferred_element_type=jnp.float32)
    up_acc = jnp.dot(scaled, w_up, preferred_element_type=jnp.float32)
    square_acc = jnp.sum(wide * wide, axis=1)
    row_scale = lax.rsqrt(square_acc / norm_gain.shape[0] + EPSILON)[:, None]
    hidden = (jax.nn.silu(gate_acc * row_scale) * (up_acc * row_scale)).astype(jnp.bfloat16)
    partial_out = jnp.dot(hidden, w_down, preferred_element_type=jnp.float32)
    summed = lax.psum_scatter(partial_out, ("kv", "tp"), scatter_dimension=1, tiled=True)
    return (stream.astype(jnp.float32) + 0.5 * summed).astype(jnp.bfloat16)


def wide_body(
    stream,
    old_state,
    decay_amounts,
    first_gain,
    first_gate,
    first_up,
    first_down,
    mixer_gain,
    query_weight,
    key_weight,
    decay_weight,
    value_weight,
    output_gate_weight,
    head_gain,
    output_weight,
    second_gain,
    second_gate,
    second_up,
    second_down,
):
    middle = half_block(stream, first_gain, first_gate, first_up, first_down)
    paired_cols = lax.all_gather(middle, "tp", axis=1, tiled=True)
    wide_cols = paired_cols.astype(jnp.float32)
    scaled = (wide_cols * mixer_gain).astype(jnp.bfloat16)
    query_part = jnp.dot(scaled, query_weight, preferred_element_type=jnp.float32)
    key_part = jnp.dot(scaled, key_weight, preferred_element_type=jnp.float32)
    decay_part = jnp.dot(scaled, decay_weight, preferred_element_type=jnp.float32)
    value_part = jnp.dot(scaled, value_weight, preferred_element_type=jnp.float32)
    outgate_part = jnp.dot(scaled, output_gate_weight, preferred_element_type=jnp.float32)
    local_rows = old_state.shape[0]
    local_heads = old_state.shape[1]
    key_dim = old_state.shape[2]
    value_dim = old_state.shape[3]
    query_sum, key_sum, decay_sum, value_sum, outgate_sum, own_squares = (
        lax.psum_scatter(query_part, "kv", scatter_dimension=0, tiled=True),
        lax.psum_scatter(key_part, "kv", scatter_dimension=0, tiled=True),
        lax.psum_scatter(decay_part, "kv", scatter_dimension=0, tiled=True),
        lax.psum_scatter(value_part, "kv", scatter_dimension=0, tiled=True),
        lax.psum_scatter(outgate_part, "kv", scatter_dimension=0, tiled=True),
        lax.psum_scatter(
            jnp.sum(wide_cols * wide_cols, axis=1), "kv", scatter_dimension=0, tiled=True
        ),
    )
    row_scale = lax.rsqrt(own_squares / (wide_cols.shape[1] * lax.axis_size("kv")) + EPSILON)[:, None]
    query = (query_sum * row_scale * key_dim ** (-0.5)).reshape(local_rows, local_heads, key_dim)
    keys = (key_sum * row_scale).reshape(local_rows, local_heads, key_dim)
    gate_logits = (decay_sum * row_scale).reshape(local_rows, local_heads, key_dim)
    values = (value_sum * row_scale).reshape(local_rows, local_heads, value_dim)
    decay_logarithm = jax.nn.log_sigmoid(gate_logits) / GATE_SOFTNESS - decay_amounts.reshape(
        local_rows, local_heads, key_dim
    )
    new_state = (
        jnp.exp(decay_logarithm)[..., None] * old_state + keys[..., None] * values[:, :, None, :]
    )
    readout = jnp.einsum("bhk,bhkv->bhv", query, new_state, precision=lax.Precision.HIGHEST)
    normed = readout * lax.rsqrt(jnp.mean(readout * readout, axis=-1, keepdims=True) + EPSILON)
    mixed_heads = (
        normed.reshape(local_rows, local_heads * value_dim)
        * head_gain
        * jax.nn.silu(outgate_sum * row_scale)
    ).astype(jnp.bfloat16)
    projected = jnp.dot(
        lax.all_gather(mixed_heads, "kv", axis=0, tiled=True),
        output_weight,
        preferred_element_type=jnp.float32,
    ).astype(jnp.bfloat16)
    attention_out = lax.psum_scatter(
        lax.optimization_barrier(projected).astype(jnp.float32).astype(jnp.bfloat16),
        "tp",
        scatter_dimension=1,
        tiled=True,
    ).astype(jnp.float32)
    after = (middle.astype(jnp.float32) + attention_out).astype(jnp.bfloat16)
    mixed_stream = half_block(after, second_gain, second_gate, second_up, second_down)
    return (mixed_stream, new_state)


def solution(mesh):
    n_kv, n_tp = mesh.shape["kv"], mesh.shape["tp"]
    few = n_kv <= 8 and n_kv & (n_kv - 1) == 0 and n_tp == 2
    program = functools.partial(body, n_kv, n_tp) if few else wide_body
    in_specs = (
        P("dp", ("kv", "tp")),
        P(("dp", "kv"), "tp", None, None),
        P(("dp", "kv"), "tp"),
        P(),
        P(None, ("kv", "tp")),
        P(None, ("kv", "tp")),
        P(("kv", "tp"), None),
        P("kv"),
        P("kv", "tp"),
        P("kv", "tp"),
        P("kv", "tp"),
        P("kv", "tp"),
        P("kv", "tp"),
        P("tp"),
        P("tp", "kv"),
        P(),
        P(None, ("kv", "tp")),
        P(None, ("kv", "tp")),
        P(("kv", "tp"), None),
    )
    out_specs = (P("dp", ("kv", "tp")), P(("dp", "kv"), "tp", None, None))
    return jax.shard_map(program, mesh=mesh, in_specs=in_specs, out_specs=out_specs, check_vma=False)
```
